32 devices in a mesh: sp: 4 (over z), fs: 4 (over y, x), tp: 2 (over core).
Axes of the slice: x: 2, y: 2, z: 4, core: 2. Of those that a mesh axis runs over, the one named last changes fastest.
Arguments:
- inputs: bfloat16 [4, 2048, 2048], P('fs', 'sp', 'tp'), may hold values from -6 to 6
- norm_gain: float32 [2048], replicated, may hold values from 0.1 to 1.9
- query_weight: bfloat16 [2048, 1024], P(('sp', 'fs'), 'tp'), may hold values from -0.125 to 0.125
- key_weight: bfloat16 [2048, 1024], P(('sp', 'fs'), 'tp'), may hold values from -0.125 to 0.125
- value_weight: bfloat16 [2048, 1024], P(('sp', 'fs'), 'tp'), may hold values from -0.125 to 0.125
- query_gain: float32 [64], replicated, may hold values from 0.8 to 7
- key_gain: float32 [64], replicated, may hold values from 0.8 to 7
- mix_lambda: float32 [8], replicated, may hold values from 0.3 to 0.8
- head_gain: float32 [128], replicated, may hold values from 0.1 to 1.9
- post_gate_weight: bfloat16 [2048, 2048], P(('sp', 'fs'), 'tp'), may hold values from -0.125 to 0.125
- pre_gate_weight: bfloat16 [2048, 2048], P(('sp', 'fs'), 'tp'), may hold values from -0.125 to 0.125
- inner_weight: bfloat16 [2048, 2048], P(('sp', 'fs'), 'tp'), may hold values from -0.125 to 0.125
- conv_taps: float32 [3, 2048], replicated, may hold values from -3 to 3
- attn_out_weight: bfloat16 [2048, 1024], P(('sp', 'fs'), 'tp'), may hold values from -0.109375 to 0.109375
- conv_out_weight: bfloat16 [2048, 2048], P(('sp', 'fs'), 'tp'), may hold values from -0.109375 to 0.109375
Outputs:
- mixed: bfloat16 [4, 2048, 2048], P('fs', ('sp', 'tp'))
The draws below stay inside these ranges and needn't reach their ends.
All inputs are finite; a program needn't handle non-finite values.
Results may differ from the reference program's by a relative error of at most 0.015.
The reference program's roundings to bfloat16 on the way count: a program that leaves them out, or rounds other values in their place, can miss the bound.
Values may be sent and summed in bfloat16 or wider, within the bound.
A program may use at most 128 MiB of HBM per device.

```python
import math
import jax
import jax.numpy as jnp
from jax import lax

D = 2048
HEADS = 8
HALF = 64
VDIM = 128
LENGTH = 2048
SEQS = 4
N_TP = 2


def gain_draw(key, salt):
    lowest = 0.8
    highest = 1.8
    fraction = jax.random.uniform(jax.random.fold_in(key, salt), (HALF,), jnp.float32)
    return jnp.exp(jnp.log(lowest) + fraction * (jnp.log(highest) - jnp.log(lowest)))


def draw_query_gain(key, part):
    return gain_draw(key, 31)


def draw_key_gain(key, part):
    return gain_draw(key, 57)


def steps_of(own_key, shape, pieces, least, largest):
    level, own = 1.0, jax.random.fold_in(own_key, 6)
    for dim, parts in pieces:
        draws = jnp.exp(jax.random.uniform(jax.random.fold_in(own, dim), (parts,), jnp.float32, least / len(pieces), largest / len(pieces)))
        level = level * jnp.repeat(draws, shape[dim] // parts).reshape([-1 if axis == dim else 1 for axis in range(len(shape))])
    return level


def centred(rng, extent, scale, most, cuts=(), kind=jnp.bfloat16):
    values = jax.random.normal(rng, extent, jnp.float32) * scale
    if len(cuts) > 0:
        values = steps_of(rng, extent, cuts, -0.22, 0.18) * values
    return jnp.clip(values, min=-most, max=most).astype(kind)


def setup_inputs(seed: int = 0) -> dict:
    keys = jax.random.split(jax.random.key(seed), 16)
    return {
        "inputs": centred(keys[0], (SEQS, LENGTH, D), 1.0, 6.0, ((0, 4), (1, 4), (2, 2))),
        "norm_gain": jnp.clip(1.0 + 0.18 * jax.random.normal(keys[1], (D,), jnp.float32), 0.1, 1.9),
        "query_weight": centred(keys[2], (D, HEADS * 2 * HALF), D ** -0.5, 0.125, ((0, 16), (1, 2))),
        "key_weight": centred(keys[3], (D, HEADS * 2 * HALF), D ** -0.5, 0.125, ((0, 16), (1, 2))),
        "value_weight": centred(keys[4], (D, HEADS * VDIM), D ** -0.5, 0.125, ((0, 16), (1, 2))),
        "query_gain": draw_query_gain(jax.random.fold_in(keys[15], 71), 0),
        "key_gain": draw_key_gain(jax.random.fold_in(keys[15], 71), 0),
        "mix_lambda": jnp.clip(jax.random.uniform(keys[7], (HEADS,), jnp.float32, 0.3, 0.8), 0.3, 0.8),
        "head_gain": jnp.clip(1.0 + 0.18 * jax.random.normal(keys[8], (VDIM,), jnp.float32), 0.1, 1.9),
        "post_gate_weight": centred(keys[9], (D, D), D ** -0.5, 0.125, ((0, 16), (1, 2))),
        "pre_gate_weight": centred(keys[10], (D, D), D ** -0.5, 0.125, ((0, 16), (1, 2))),
        "inner_weight": centred(keys[11], (D, D), D ** -0.5, 0.125, ((0, 16), (1, 2))),
        "conv_taps": centred(keys[12], (3, D), 0.6, 3.0, (), jnp.float32),
        "attn_out_weight": centred(keys[13], (D, HEADS * VDIM), (HEADS * VDIM + D) ** -0.5, 0.109375, ((0, 16), (1, 2))),
        "conv_out_weight": centred(keys[14], (D, D), (HEADS * VDIM + D) ** -0.5, 0.109375, ((0, 16), (1, 2))),
    }


epsilon = 1e-06

def scale_rows(values, gain):
    return values * lax.rsqrt(lax.optimization_barrier(jnp.mean(values * values, axis=-1, keepdims=True)) + epsilon) * gain

def attend_head(query_head, key_head, value_head, weight_two):
    block = math.gcd(LENGTH, 512)
    query_blocks = jnp.transpose(query_head.reshape(2, LENGTH // block, block, HALF), (1, 0, 2, 3))
    keys_wide = key_head.astype(jnp.float32)
    values_wide = value_head.astype(jnp.float32)

    def one_block(query_block):
        scores = jnp.einsum('jqd,jkd->jqk', query_block.astype(jnp.float32), keys_wide) * HALF ** (-0.5)
        peak = lax.optimization_barrier(jnp.max(scores, axis=-1, keepdims=True))
        expo = jnp.exp(scores - peak)
        total = lax.optimization_barrier(jnp.sum(expo, axis=-1, keepdims=True))
        rounded = lax.optimization_barrier(expo.astype(jnp.bfloat16)).astype(jnp.float32)
        mapped = jnp.einsum('jqk,kd->jqd', rounded, values_wide) / total
        return mapped[0] - weight_two * mapped[1]
    result = lax.map(one_block, query_blocks)
    return result.reshape(LENGTH, VDIM)

def one_sequence(tokens, norm_gain, query_weight, key_weight, value_weight, query_gain, key_gain, mix_lambda, head_gain, post_gate_weight, pre_gate_weight, inner_weight, conv_taps, attn_out_weight, conv_out_weight):
    normed = scale_rows(tokens.astype(jnp.float32), norm_gain).astype(jnp.bfloat16)
    query = jnp.dot(normed, query_weight, preferred_element_type=jnp.float32).reshape(LENGTH, HEADS, 2, HALF)
    key = jnp.dot(normed, key_weight, preferred_element_type=jnp.float32).reshape(LENGTH, HEADS, 2, HALF)
    query_normed = scale_rows(query, query_gain).astype(jnp.bfloat16)
    key_normed = scale_rows(key, key_gain).astype(jnp.bfloat16)
    values = jnp.dot(normed, value_weight, preferred_element_type=jnp.float32).astype(jnp.bfloat16)
    values = values.reshape(LENGTH, HEADS, VDIM)

    def per_head(members):
        return attend_head(members[0], members[1], members[2], members[3])
    head_out = lax.map(per_head, (jnp.transpose(query_normed, (1, 2, 0, 3)), jnp.transpose(key_normed, (1, 2, 0, 3)), jnp.transpose(values, (1, 0, 2)), mix_lambda))
    attn_hidden = scale_rows(head_out, head_gain).astype(jnp.bfloat16)
    attn_hidden = jnp.transpose(attn_hidden, (1, 0, 2)).reshape(LENGTH, HEADS * VDIM)
    post = jnp.dot(normed, post_gate_weight, preferred_element_type=jnp.float32).astype(jnp.bfloat16)
    post_wide = lax.optimization_barrier(post).astype(jnp.float32)
    signal = (jnp.dot(normed, pre_gate_weight, preferred_element_type=jnp.float32) * jnp.dot(normed, inner_weight, preferred_element_type=jnp.float32)).astype(jnp.bfloat16)
    padded = jnp.pad(lax.optimization_barrier(signal).astype(jnp.float32), ((1, 1), (0, 0)))
    filtered = conv_taps[0] * padded[:-2] + conv_taps[1] * padded[1:-1] + conv_taps[2] * padded[2:]
    conv_hidden = (post_wide * filtered).astype(jnp.bfloat16)
    head_span = HEADS // N_TP * VDIM
    channel_span = D // N_TP
    summed = jnp.zeros((LENGTH, D), jnp.float32)
    for group in range(N_TP):
        attn_part = attn_hidden[:, group * head_span:(group + 1) * head_span]
        attn_cols = attn_out_weight[:, group * head_span:(group + 1) * head_span]
        conv_part = conv_hidden[:, group * channel_span:(group + 1) * channel_span]
        conv_cols = conv_out_weight[:, group * channel_span:(group + 1) * channel_span]
        partial_value = jnp.dot(attn_part, attn_cols.T, preferred_element_type=jnp.float32) + jnp.dot(conv_part, conv_cols.T, preferred_element_type=jnp.float32)
        summed = summed + lax.optimization_barrier(partial_value.astype(jnp.bfloat16)).astype(jnp.float32)
    return summed.astype(jnp.bfloat16)

def reference(inputs, norm_gain, query_weight, key_weight, value_weight, query_gain, key_gain, mix_lambda, head_gain, post_gate_weight, pre_gate_weight, inner_weight, conv_taps, attn_out_weight, conv_out_weight):
    results = []
    for sequence in range(SEQS):
        results.append(one_sequence(inputs[sequence], norm_gain, query_weight, key_weight, value_weight, query_gain, key_gain, mix_lambda, head_gain, post_gate_weight, pre_gate_weight, inner_weight, conv_taps, attn_out_weight, conv_out_weight))
    return jnp.stack(results, axis=0)
```

```python
import math

import jax
import jax.numpy as jnp
from jax import lax
from jax.experimental import pallas as pl
from jax.experimental.pallas import tpu as pltpu
from jax.sharding import PartitionSpec as P

epsilon = 1e-06


def padded_2(x, sides, width):
    for axis, dim in sides:
        size, length = (lax.axis_size(axis), x.shape[dim])
        up = [(i, (i + 1) % size) for i in range(size - 1)]
        down = [(j, i) for i, j in up]
        last = lax.slice_in_dim(x, length - width, length, axis=dim)
        initial = lax.slice_in_dim(x, 0, width, axis=dim)
        before = lax.ppermute(last, axis, up)
        after = lax.ppermute(initial, axis, down)
        x = jnp.concatenate([before, x, after], axis=dim)
    return x


def scale_rows(values, gain):
    return values * lax.rsqrt(jnp.mean(values * values, axis=-1, keepdims=True) + epsilon) * gain


def project_all(normed, weights, products):
    result = []
    for member in range(len(weights)):
        if member < products:
            result.append(jnp.dot(normed, weights[member], preferred_element_type=jnp.float32))
        else:
            result.append(weights[member])
    return tuple(result)


def attention_branch(query, key, values, weight_two, query_gain, key_gain, head_gain):
    tok_rows = query.shape[0]
    vsize = head_gain.shape[0]
    half = query_gain.shape[0]
    heads = values.shape[1] // vsize
    query_normed = scale_rows(query.reshape(tok_rows, heads, 2, half), query_gain).astype(
        jnp.bfloat16
    )
    key_normed = scale_rows(key.reshape(tok_rows, heads * 2, half), key_gain).astype(jnp.bfloat16)
    key_normed = key_normed.reshape(tok_rows, heads * 2 * half)
    scale = half ** (-0.5)
    initial = (
        jnp.full((heads, 2, tok_rows), -1e30, jnp.float32),
        jnp.zeros((heads, 2, tok_rows), jnp.float32),
        jnp.zeros((heads, 2, tok_rows, vsize), jnp.float32),
    )
    carry = initial
    key_piece = lax.all_gather(key_normed, "sp", axis=0, tiled=True)
    value_piece = lax.all_gather(values, "sp", axis=0, tiled=True)
    length = key_piece.shape[0]
    block = math.gcd(length, 512)
    key_blocks = key_piece.reshape(length // block, block, heads, 2, half)
    value_blocks = value_piece.reshape(length // block, block, heads, vsize)

    def one_block(state, blocks):
        peak, total, accum = state
        key_block, value_block = blocks
        scores = (
            jnp.einsum(
                "qhjd,khjd->hjqk", query_normed, key_block, preferred_element_type=jnp.float32
            )
            * scale
        )
        new_peak = jnp.maximum(peak, jnp.max(scores, axis=-1))
        factor = jnp.exp(peak - new_peak)
        expo = jnp.exp(scores - new_peak[..., None])
        total = total * factor + jnp.sum(expo, axis=-1)
        accum = accum * factor[..., None] + jnp.einsum(
            "hjqk,khd->hjqd",
            expo.astype(jnp.bfloat16),
            value_block,
            preferred_element_type=jnp.float32,
        )
        return ((new_peak, total, accum), None)

    carry, unused = lax.scan(one_block, carry, (key_blocks, value_blocks))
    peak, total, accum = carry
    mapped = accum / total[..., None]
    head_out = mapped[:, 0] - weight_two[:, None, None] * mapped[:, 1]
    normed_out = scale_rows(head_out, head_gain).astype(jnp.bfloat16)
    return jnp.transpose(normed_out, (1, 0, 2)).reshape(tok_rows, heads * vsize)


def half_scaled(values, gain, half):
    low = lax.broadcasted_iota(jnp.int32, (1, 2 * half), 1) < half
    squares = values * values
    first = jnp.sum(jnp.where(low, squares, 0.0), axis=-1, keepdims=True) / half
    second = jnp.sum(jnp.where(low, 0.0, squares), axis=-1, keepdims=True) / half
    factor = jnp.where(low, lax.rsqrt(first + epsilon), lax.rsqrt(second + epsilon))
    return values * factor * gain


def remote(source, target, send, recv, where):
    return pltpu.make_async_remote_copy(
        src_ref=source,
        dst_ref=target,
        send_sem=send,
        recv_sem=recv,
        device_id=where,
        device_id_type=pl.DeviceIdType.MESH,
    )


def meet(places):
    barrier = pltpu.get_barrier_semaphore()
    for where in places:
        pl.semaphore_signal(
            barrier, inc=1, device_id=where, device_id_type=pl.DeviceIdType.MESH
        )
    pl.semaphore_wait(barrier, len(places))


def load(source, target, sem):
    return pltpu.make_async_copy(source, target, sem)


def choose(table, z):
    value = table[0]
    for at in range(1, len(table)):
        value = jnp.where(z == at, table[at], value)
    return value


def fused_kernel(
    n, half, tok_ref, q_ref, k_ref, v_ref, post_ref, pre_ref, inner_ref, ao_ref, co_ref,
    gain_ref, qg_ref, kg_ref, lam_ref, hg_ref, taps_ref, out_ref,
    pack, w_all, t_raw, t_twin, t_all, o_raw, wo_all, query, key, val, post, signal, conv_hid,
    attn_hid, hin, mine, give, take,
    l_sem, z_send, z_recv, f_send, f_recv, g_send, g_recv, r_send, r_recv, t_send, t_recv,
    p_send, p_recv, o_send, o_recv, of_send, of_recv, og_send, og_recv, c_send, c_recv,
    a_send, a_recv, e_send, e_recv,
):
    z, f, c = lax.axis_index("sp"), lax.axis_index("fs"), lax.axis_index("tp")
    beside, above = f + 1 - 2 * (f % 2), f + 2 - 4 * (f // 2)
    near = sorted(range(1, n), key=lambda d: min(d, n - d))
    fs = wo_all.shape[0] // n
    rows = tok_ref.shape[0]
    w_rows = q_ref.shape[0]
    total_rows = rows * n
    vsize = v_ref.shape[1] // n
    channels = post_ref.shape[1] // n
    wide = 2 * half
    o_attn = ao_ref.shape[1]
    bf16, f32 = jnp.bfloat16, jnp.float32

    members = ((q_ref, wide), (k_ref, wide), (pre_ref, channels), (inner_ref, channels),
               (post_ref, channels), (v_ref, vsize))
    starts = [0]
    for ref, width in members:
        starts.append(starts[-1] + width)

    def w_place(s, g):
        return w_all.at[pl.ds(pl.multiple_of((s * fs + g) * w_rows, w_rows), w_rows)]

    tok_load = load(tok_ref, t_raw, l_sem.at[n * 6])
    tok_load.start()
    loads = {}
    for d in near + [0]:
        to = (z + d) % n
        target = pack.at[d] if d else w_place(z, f)
        loads[d] = []
        for m, (ref, width) in enumerate(members):
            piece = load(
                ref.at[:, pl.ds(pl.multiple_of(to * width, width), width)],
                target.at[:, pl.ds(starts[m], width)],
                l_sem.at[d * 6 + m],
            )
            piece.start()
            loads[d].append(piece)
    o_loads = [
        load(ao_ref, o_raw.at[:, pl.ds(0, o_attn)], l_sem.at[n * 6 + 1]),
        load(co_ref, o_raw.at[:, pl.ds(o_attn, co_ref.shape[1])], l_sem.at[n * 6 + 2]),
    ]
    for piece in o_loads:
        piece.start()

    meet([{"sp": (z + d) % n} for d in near] + [{"fs": beside}, {"fs": above}, {"tp": 1 - c}])

    flights = []

    def go(copy):
        copy.start()
        flights.append(copy)
        return copy

    tok_load.wait()
    raw = go(remote(t_raw, t_twin, r_send.at[0], r_recv.at[0], {"tp": 1 - c}))
    across = {}
    for d in near:
        for piece in loads[d]:
            piece.wait()
        across[d] = go(
            remote(pack.at[d], w_place(z, f), z_send.at[d], z_recv.at[d], {"sp": (z + d) % n})
        )
    for piece in loads[0]:
        piece.wait()
    side = {}

    def spread(d):
        s = (z + n - d) % n
        for i, to in enumerate((beside, above)):
            side[i, d] = go(
                remote(w_place(s, f), w_place(s, f), f_send.at[i, d], f_recv.at[i, d], {"fs": to})
            )

    further = {}

    def pass_on(d):
        s = (z + n - d) % n
        i = d % 2
        side[i, d].wait_recv()
        held, to = (beside, above) if i == 0 else (above, beside)
        further[d] = go(
            remote(w_place(s, held), w_place(s, held), g_send.at[d], g_recv.at[d], {"fs": to})
        )

    spread(0)

    raw.wait_recv()
    tile = math.gcd(rows, 64)

    def norm_rows(i, unused):
        at = pl.ds(pl.multiple_of(i * tile, tile), tile)
        to = pl.ds(pl.multiple_of(z * rows + i * tile, tile), tile)
        own, twin = t_raw[at, :].astype(f32), t_twin[at, :].astype(f32)
        square = jnp.sum(own * own, axis=-1, keepdims=True) + jnp.sum(
            twin * twin, axis=-1, keepdims=True
        )
        factor = lax.rsqrt(square / (2 * own.shape[1]) + epsilon)
        t_all[c, to, :] = (own * factor * gain_ref[c]).astype(bf16)
        t_all[1 - c, to, :] = (twin * factor * gain_ref[1 - c]).astype(bf16)
        return unused

    lax.fori_loop(0, rows // tile, norm_rows, 0)

    def t_place(s):
        return t_all.at[c, pl.ds(pl.multiple_of(s * rows, rows), rows)]

    def t_along(s, step):
        return remote(
            t_place(s), t_place(s), t_send.at[(step + 1) // 2, s], t_recv.at[s], {"sp": z + step}
        )

    def t_aside(s):
        return remote(t_place(s), t_place(s), p_send.at[s], p_recv.at[s], {"tp": 1 - c})

    def o_place(s, g):
        return wo_all.at[s * fs + g]

    def o_along(s, step):
        return remote(
            o_place(s, f), o_place(s, f), o_send.at[(step + 1) // 2, s], o_recv.at[s],
            {"sp": z + step},
        )

    def o_side(s, i):
        return remote(
            o_place(s, f), o_place(s, f), of_send.at[i, s], of_recv.at[i, s],
            {"fs": (beside, above)[i]},
        )

    def o_further(s, d):
        held, to = (beside, above) if d % 2 == 0 else (above, beside)
        return remote(
            o_place(s, held), o_place(s, held), og_send.at[s], og_recv.at[s], {"fs": to}
        )

    def both_ways(along):
        for step in (1, -1):
            @pl.when(jnp.logical_and(z + step >= 0, z + step < n))
            def _(step=step):
                along(z, step).start()

    both_ways(t_along)

    for piece in o_loads:
        piece.wait()
    square = o_raw.shape[0]
    for i in range(o_raw.shape[1] // square):
        wo_all[z * fs + f, i * square:(i + 1) * square, :] = o_raw[
            :, i * square:(i + 1) * square
        ].T
    both_ways(o_along)

    last = 0
    for d in near:
        across[d].wait_recv()
        spread(d)
        pass_on(last)
        last = d
    pass_on(last)
    for i in range(2):
        o_side(z, i).start()
    for d in range(n):
        side[1 - d % 2, d].wait_recv()
        further[d].wait_recv()

    order = [sorted(range(n), key=lambda s: (abs(s - at), s > at if 2 * at < n else s < at))
             for at in range(n)]

    def t_event(at, s):
        t_along(s, 1).wait_recv()
        step = 1 if s < at else -1
        if 0 <= at + step < n:
            t_along(s, step).start()
        t_aside(s).start()

    def o_event(at, s):
        o_along(s, 1).wait_recv()
        step = 1 if s < at else -1
        if 0 <= at + step < n:
            o_along(s, step).start()
        for i in range(2):
            o_side(s, i).start()

    def o_pass(at, s):
        d = (at - s) % n
        o_side(s, d % 2).wait_recv()
        o_further(s, d).start()

    plans = []
    for at in range(n):
        plan = [[] for _ in range(n + 1)]
        t_done, o_done, p_done = {at}, {at}, set()
        for visit in range(1, n):
            s = order[at][visit]
            for r in order[at]:
                if abs(r - at) < abs(s - at) and r not in o_done:
                    plan[visit].append((o_event, r))
                    o_done.add(r)
            if s not in t_done:
                for r in order[at]:
                    if abs(r - at) == abs(s - at):
                        plan[visit].append((t_event, r))
                        t_done.add(r)
            elif s not in o_done:
                for r in order[at]:
                    if abs(r - at) == abs(s - at):
                        plan[visit].append((o_event, r))
                        o_done.add(r)
            ready = [r for r in order[at] if r in o_done and r not in p_done]
            if visit == 1 or visit == n - 1:
                for r in ready:
                    plan[visit].append((o_pass, r))
                    p_done.add(r)
        for r in order[at]:
            if r not in o_done:
                plan[n - 1 + 1].append((o_event, r))
        plans.append((plan, [r for r in order[at] if r not in p_done]))

    def follow(stage):
        for at in range(n):
            if plans[at][0][stage]:
                @pl.when(z == at)
                def _(at=at):
                    for event, s in plans[at][0][stage]:
                        event(at, s)

    deep = t_all.shape[2]
    m_rows = math.gcd(rows, 256)

    def project(s):
        def some(i, unused):
            base = pl.multiple_of(s * rows + i * m_rows, m_rows)
            at = pl.ds(base, m_rows)

            def product(first, final):
                lo, hi = starts[first], starts[final]
                return jnp.dot(
                    t_all[0, at, :], w_all[0:deep, lo:hi], preferred_element_type=f32
                ) + jnp.dot(
                    t_all[1, at, :], w_all[deep:2 * deep, lo:hi], preferred_element_type=f32
                )

            pair = product(0, 2)
            low = lax.broadcasted_iota(jnp.int32, (1, wide), 1) < half
            q = half_scaled(pair[:, :wide], qg_ref[...], half).astype(bf16).astype(f32)
            query[0, at, :] = jnp.where(low, q, 0.0).astype(bf16)
            query[1, at, :] = jnp.where(low, 0.0, q).astype(bf16)
            key[at, :] = half_scaled(pair[:, wide:], kg_ref[...], half).astype(bf16)
            mixed = product(2, 3) * product(3, 4)
            signal[pl.ds(base + 8, m_rows), :] = mixed.astype(bf16).astype(f32)
            post[at, :] = product(4, 5).astype(bf16)
            val[at, :] = product(5, 6).astype(bf16)
            return unused

        lax.fori_loop(0, rows // m_rows, some, 0)

    signal[0:8, :] = jnp.zeros((8, channels), f32)
    signal[total_rows + 8:total_rows + 16, :] = jnp.zeros((8, channels), f32)
    project(z)
    for visit in range(1, n):
        follow(visit)
        s = choose([order[at][visit] for at in range(n)], z)
        t_aside(s).wait_recv()
        project(s)

    place = c * n + z
    taps = taps_ref[:, pl.ds(pl.multiple_of(place * channels, channels), channels)]
    h_rows = math.gcd(rows, 64)

    def convolve(i, unused):
        base = pl.multiple_of(i * h_rows, h_rows)
        around = signal[pl.ds(base, h_rows + 16), :]
        before = around[7:7 + h_rows]
        middle = around[8:8 + h_rows]
        after = around[9:9 + h_rows]
        filtered = taps[0:1] * before + taps[1:2] * middle + taps[2:3] * after
        at = pl.ds(base, h_rows)
        conv_hid[at, :] = (post[at, :].astype(f32) * filtered).astype(bf16)
        return unused

    lax.fori_loop(0, total_rows // h_rows, convolve, 0)
    conv_at = pl.ds(pl.multiple_of(o_attn + z * channels, channels), channels)
    attn_at = pl.ds(pl.multiple_of(z * vsize, vsize), vsize)

    def c_copy(d):
        to = (z + d) % n
        return remote(
            conv_hid.at[pl.ds(pl.multiple_of(to * rows, rows), rows)], hin.at[:, conv_at],
            c_send.at[d], c_recv.at[d], {"sp": to},
        )

    def a_copy(d):
        to = (z + d) % n
        return remote(
            attn_hid.at[pl.ds(pl.multiple_of(to * rows, rows), rows)], hin.at[:, attn_at],
            a_send.at[d], a_recv.at[d], {"sp": to},
        )

    far = near[::-1]
    for d in far:
        c_copy(d).start()
    own = pl.ds(pl.multiple_of(z * rows, rows), rows)
    hin[:, conv_at] = conv_hid[own, :]

    a_rows = math.gcd(rows, 256)
    each = rows // a_rows
    scale = half ** (-0.5) * math.log2(math.e)
    lam = lam_ref[place]

    def attend(i, unused):
        @pl.when(i == 2)
        def _():
            follow(n)

        d = choose(far + [0], i // each)
        at = pl.ds(pl.multiple_of(((z + d) % n) * rows + (i % each) * a_rows, a_rows), a_rows)
        maps = []
        for which in range(2):
            scores = lax.dot_general(
                query[which, at, :], key[...], (((1,), (1,)), ((), ())),
                preferred_element_type=f32,
            ) * scale
            expo = jnp.exp2(scores - jnp.max(scores, axis=-1, keepdims=True))
            total = jnp.sum(expo, axis=-1, keepdims=True)
            maps.append(
                jnp.dot(expo.astype(bf16), val[...], preferred_element_type=f32) / total
            )
        head_out = maps[0] - lam * maps[1]
        attn_hid[at, :] = scale_rows(head_out, hg_ref[...]).astype(bf16)
        for j, d in enumerate(far):
            @pl.when(i == (j + 1) * each - 1)
            def _(d=d):
                a_copy(d).start()
        return unused

    lax.fori_loop(0, n * each, attend, 0)
    hin[:, attn_at] = attn_hid[own, :]
    for at in range(n):
        @pl.when(z == at)
        def _(at=at):
            for s in plans[at][1]:
                o_pass(at, s)

    for s in range(n):
        for i in range(2):
            @pl.when((z + n - s) % 2 != i)
            def _(s=s, i=i):
                o_side(s, i).wait_recv()
        o_further(s, 0).wait_recv()
    for d in far:
        c_copy(d).wait_recv()
        a_copy(d).wait_recv()

    pairs = wo_all.shape[0] // 2
    half_rows = rows // 2

    def swap(j):
        return remote(give.at[j], take.at[j], e_send.at[j], e_recv.at[j], {"tp": 1 - c})

    def produce(j, unused):
        weights = jnp.concatenate([wo_all[2 * j], wo_all[2 * j + 1]], axis=1)
        theirs = pl.ds(pl.multiple_of((1 - c) * half_rows, half_rows), half_rows)
        ours = pl.ds(pl.multiple_of(c * half_rows, half_rows), half_rows)
        give[j] = jnp.dot(hin[theirs, :], weights, preferred_element_type=f32).astype(bf16)
        swap(j).start()
        mine[j] = jnp.dot(hin[ours, :], weights, preferred_element_type=f32).astype(bf16)
        return unused

    lax.fori_loop(0, pairs, produce, 0)
    width = give.shape[2]

    for j in range(pairs):
        swap(j).wait_recv()
        out_ref[:, j * width:(j + 1) * width] = (
            mine[j].astype(f32) + take[j].astype(f32)
        ).astype(bf16)

    for copy in flights:
        copy.wait_send()
    for d in far:
        c_copy(d).wait_send()
        a_copy(d).wait_send()
    for j in range(pairs):
        swap(j).wait_send()
    for s in range(n):
        for i in range(2):
            o_side(s, i).wait_send()
        o_further(s, 0).wait_send()
        for step in (1, -1):
            arrives = s <= z if step == 1 else s >= z
            @pl.when(jnp.logical_and(arrives, jnp.logical_and(z + step >= 0, z + step < n)))
            def _(s=s, step=step):
                t_along(s, step).wait_send()
                o_along(s, step).wait_send()

        @pl.when(z != s)
        def _(s=s):
            t_aside(s).wait_send()


def split_device(
    inputs,
    norm_gain,
    query_weight,
    key_weight,
    value_weight,
    query_gain,
    key_gain,
    mix_lambda,
    head_gain,
    post_gate_weight,
    pre_gate_weight,
    inner_weight,
    conv_taps,
    attn_out_weight,
    conv_out_weight,
):
    n, fs, tp = lax.axis_size("sp"), lax.axis_size("fs"), lax.axis_size("tp")
    tokens = inputs[0]
    rows, deep = tokens.shape
    half, vsize = query_gain.shape[0], head_gain.shape[0]
    channels = post_gate_weight.shape[1] // n
    w_rows = query_weight.shape[0]
    columns = 4 * half + vsize + 3 * channels
    hidden = n * (vsize + channels)
    total = n * rows
    out_width = w_rows * n * fs
    pairs = n * fs // 2
    bf16, dma = jnp.bfloat16, pltpu.SemaphoreType.DMA
    far, close = pl.BlockSpec(memory_space=pl.ANY), pl.BlockSpec(memory_space=pltpu.VMEM)
    result = pl.pallas_call(
        lambda *refs: fused_kernel(n, half, *refs),
        out_shape=jax.ShapeDtypeStruct((rows // tp, out_width), bf16),
        in_specs=[far] * 9 + [close] * 3 + [pl.BlockSpec(memory_space=pltpu.SMEM)] + [close] * 2,
        out_specs=close,
        scratch_shapes=[
            pltpu.VMEM((n, w_rows, columns), bf16),
            pltpu.VMEM((n * fs * w_rows, columns), bf16),
            pltpu.VMEM((rows, deep), bf16),
            pltpu.VMEM((rows, deep), bf16),
            pltpu.VMEM((tp, total, deep), bf16),
            pltpu.VMEM((w_rows, hidden), bf16),
            pltpu.VMEM((n * fs, hidden, w_rows), bf16),
            pltpu.VMEM((2, total, 2 * half), bf16),
            pltpu.VMEM((total, 2 * half), bf16),
            pltpu.VMEM((total, vsize), bf16),
            pltpu.VMEM((total, channels), bf16),
            pltpu.VMEM((total + 16, channels), jnp.float32),
            pltpu.VMEM((total, channels), bf16),
            pltpu.VMEM((total, vsize), bf16),
            pltpu.VMEM((rows, hidden), bf16),
            pltpu.VMEM((pairs, rows // tp, 2 * w_rows), bf16),
            pltpu.VMEM((pairs, rows // tp, 2 * w_rows), bf16),
            pltpu.VMEM((pairs, rows // tp, 2 * w_rows), bf16),
            dma((n * 6 + 3,)),
            dma((n,)), dma((n,)), dma((2, n)), dma((2, n)), dma((n,)), dma((n,)),
            dma((1,)), dma((1,)), dma((2, n)), dma((n,)), dma((n,)), dma((n,)),
            dma((2, n)), dma((n,)), dma((2, n)), dma((2, n)), dma((n,)), dma((n,)),
            dma((n,)), dma((n,)), dma((n,)), dma((n,)), dma((pairs,)), dma((pairs,)),
        ],
        compiler_params=pltpu.CompilerParams(
            collective_id=1, has_side_effects=True, vmem_limit_bytes=60 * 2**20
        ),
    )(
        tokens, query_weight, key_weight, value_weight, post_gate_weight, pre_gate_weight,
        inner_weight, attn_out_weight, conv_out_weight,
        norm_gain.reshape(tp, 1, deep),
        jnp.tile(query_gain, 2)[None],
        jnp.tile(key_gain, 2)[None],
        mix_lambda,
        head_gain[None],
        conv_taps,
    )
    return result[None]


def per_device(
    inputs,
    norm_gain,
    query_weight,
    key_weight,
    value_weight,
    query_gain,
    key_gain,
    mix_lambda,
    head_gain,
    post_gate_weight,
    pre_gate_weight,
    inner_weight,
    conv_taps,
    attn_out_weight,
    conv_out_weight,
):
    tokens = inputs[0]
    whole = lax.all_gather(tokens, "tp", axis=1, tiled=True)
    normed = scale_rows(whole.astype(jnp.float32), norm_gain).astype(jnp.bfloat16)
    heads_dev = value_weight.shape[1] // head_gain.shape[0]
    channels = post_gate_weight.shape[1]
    tp_index = lax.axis_index("tp")
    weight_two = lax.dynamic_slice_in_dim(mix_lambda, tp_index * heads_dev, heads_dev)
    taps = lax.dynamic_slice_in_dim(conv_taps, tp_index * channels, channels, 1)
    every_full = (
        lax.all_gather(query_weight, ("sp", "fs"), axis=0, tiled=True),
        lax.all_gather(key_weight, ("sp", "fs"), axis=0, tiled=True),
        lax.all_gather(value_weight, ("sp", "fs"), axis=0, tiled=True),
        lax.all_gather(post_gate_weight, ("sp", "fs"), axis=0, tiled=True),
        lax.all_gather(pre_gate_weight, ("sp", "fs"), axis=0, tiled=True),
        lax.all_gather(inner_weight, ("sp", "fs"), axis=0, tiled=True),
        lax.all_gather(attn_out_weight, ("sp", "fs"), axis=0, tiled=True),
        lax.all_gather(conv_out_weight, ("sp", "fs"), axis=0, tiled=True),
    )
    query, key, value_proj, post, pre_gate, inner, attn_out_full, conv_out_full = project_all(
        normed, every_full[0:3] + every_full[3:6] + every_full[6:8], 6
    )
    attn_hidden = attention_branch(
        query, key, value_proj.astype(jnp.bfloat16), weight_two, query_gain, key_gain, head_gain
    )
    post_mid = post.astype(jnp.bfloat16)
    post_wide = lax.optimization_barrier(post_mid).astype(jnp.float32)
    signal = (pre_gate * inner).astype(jnp.bfloat16)
    padded = padded_2(signal, (("sp", 0),), 1)
    shifted = lax.optimization_barrier(padded).astype(jnp.float32)
    filtered = taps[0] * shifted[:-2] + taps[1] * shifted[1:-1] + taps[2] * shifted[2:]
    conv_hidden = (post_wide * filtered).astype(jnp.bfloat16)
    contract = (((1,), (1,)), ((), ()))
    summed = lax.psum_scatter(
        (
            lax.dot_general(
                attn_hidden, attn_out_full, contract, preferred_element_type=jnp.float32
            )
            + lax.dot_general(
                conv_hidden, conv_out_full, contract, preferred_element_type=jnp.float32
            )
        ).astype(jnp.bfloat16),
        "tp",
        scatter_dimension=0,
        tiled=True,
    )
    return summed[None]


def solution(mesh):
    placed = (
        P("fs", "sp", "tp"),
        P(),
        P(("sp", "fs"), "tp"),
        P(("sp", "fs"), "tp"),
        P(("sp", "fs"), "tp"),
        P(),
        P(),
        P(),
        P(),
        P(("sp", "fs"), "tp"),
        P(("sp", "fs"), "tp"),
        P(("sp", "fs"), "tp"),
        P(),
        P(("sp", "fs"), "tp"),
        P(("sp", "fs"), "tp"),
    )
    sp, tp = mesh.shape["sp"], mesh.shape["tp"]

    def program(*args):
        heads = args[7].shape[0]
        channels = args[12].shape[1]
        splits = tp == 2 and mesh.shape["fs"] == 4 and sp > 1 and heads == sp * tp
        splits = splits and channels % (sp * tp * 128) == 0
        return shard(split_device if splits else per_device)(*args)

    shard = lambda body: jax.shard_map(
        body,
        mesh=mesh,
        in_specs=placed,
        out_specs=P("fs", ("sp", "tp"), None),
        check_vma=False,
    )

    return program
```

```python
import math

import jax
import jax.numpy as jnp
from jax import lax
from jax.experimental import pallas as pl
from jax.experimental.pallas import tpu as pltpu
from jax.sharding import PartitionSpec as P

epsilon = 1e-06


def padded_2(x, sides, width):
    for axis, dim in sides:
        size, length = (lax.axis_size(axis), x.shape[dim])
        up = [(i, (i + 1) % size) for i in range(size - 1)]
        down = [(j, i) for i, j in up]
        last = lax.slice_in_dim(x, length - width, length, axis=dim)
        initial = lax.slice_in_dim(x, 0, width, axis=dim)
        before = lax.ppermute(last, axis, up)
        after = lax.ppermute(initial, axis, down)
        x = jnp.concatenate([before, x, after], axis=dim)
    return x


def scale_rows(values, gain):
    return values * lax.rsqrt(jnp.mean(values * values, axis=-1, keepdims=True) + epsilon) * gain


def project_all(normed, weights, products):
    result = []
    for member in range(len(weights)):
        if member < products:
            result.append(jnp.dot(normed, weights[member], preferred_element_type=jnp.float32))
        else:
            result.append(weights[member])
    return tuple(result)


def attention_branch(query, key, values, weight_two, query_gain, key_gain, head_gain):
    tok_rows = query.shape[0]
    vsize = head_gain.shape[0]
    half = query_gain.shape[0]
    heads = values.shape[1] // vsize
    query_normed = scale_rows(query.reshape(tok_rows, heads, 2, half), query_gain).astype(
        jnp.bfloat16
    )
    key_normed = scale_rows(key.reshape(tok_rows, heads * 2, half), key_gain).astype(jnp.bfloat16)
    key_normed = key_normed.reshape(tok_rows, heads * 2 * half)
    scale = half ** (-0.5)
    initial = (
        jnp.full((heads, 2, tok_rows), -1e30, jnp.float32),
        jnp.zeros((heads, 2, tok_rows), jnp.float32),
        jnp.zeros((heads, 2, tok_rows, vsize), jnp.float32),
    )
    carry = initial
    key_piece = lax.all_gather(key_normed, "sp", axis=0, tiled=True)
    value_piece = lax.all_gather(values, "sp", axis=0, tiled=True)
    length = key_piece.shape[0]
    block = math.gcd(length, 512)
    key_blocks = key_piece.reshape(length // block, block, heads, 2, half)
    value_blocks = value_piece.reshape(length // block, block, heads, vsize)

    def one_block(state, blocks):
        peak, total, accum = state
        key_block, value_block = blocks
        scores = (
            jnp.einsum(
                "qhjd,khjd->hjqk", query_normed, key_block, preferred_element_type=jnp.float32
            )
            * scale
        )
        new_peak = jnp.maximum(peak, jnp.max(scores, axis=-1))
        factor = jnp.exp(peak - new_peak)
        expo = jnp.exp(scores - new_peak[..., None])
        total = total * factor + jnp.sum(expo, axis=-1)
        accum = accum * factor[..., None] + jnp.einsum(
            "hjqk,khd->hjqd",
            expo.astype(jnp.bfloat16),
            value_block,
            preferred_element_type=jnp.float32,
        )
        return ((new_peak, total, accum), None)

    carry, unused = lax.scan(one_block, carry, (key_blocks, value_blocks))
    peak, total, accum = carry
    mapped = accum / total[..., None]
    head_out = mapped[:, 0] - weight_two[:, None, None] * mapped[:, 1]
    normed_out = scale_rows(head_out, head_gain).astype(jnp.bfloat16)
    return jnp.transpose(normed_out, (1, 0, 2)).reshape(tok_rows, heads * vsize)


def half_scaled(values, gain, half):
    low = lax.broadcasted_iota(jnp.int32, (1, 2 * half), 1) < half
    squares = values * values
    first = jnp.sum(jnp.where(low, squares, 0.0), axis=-1, keepdims=True) / half
    second = jnp.sum(jnp.where(low, 0.0, squares), axis=-1, keepdims=True) / half
    factor = jnp.where(low, lax.rsqrt(first + epsilon), lax.rsqrt(second + epsilon))
    return values * factor * gain


def remote(source, target, send, recv, where):
    return pltpu.make_async_remote_copy(
        src_ref=source,
        dst_ref=target,
        send_sem=send,
        recv_sem=recv,
        device_id=where,
        device_id_type=pl.DeviceIdType.MESH,
    )


def meet(places):
    barrier = pltpu.get_barrier_semaphore()
    for where in places:
        pl.semaphore_signal(
            barrier, inc=1, device_id=where, device_id_type=pl.DeviceIdType.MESH
        )
    pl.semaphore_wait(barrier, len(places))


def load(source, target, sem):
    return pltpu.make_async_copy(source, target, sem)


def choose(table, z):
    value = table[0]
    for at in range(1, len(table)):
        value = jnp.where(z == at, table[at], value)
    return value


def fused_kernel(
    n, half, tok_ref, q_ref, k_ref, v_ref, post_ref, pre_ref, inner_ref, ao_ref, co_ref,
    ng_any, qg_any, kg_any, lam_ref, hg_any, taps_any, mine, take,
    gain_ref, qg_ref, kg_ref, hg_ref, taps_ref, acc, pack, w_all, t_raw, t_twin, t_all, o_raw, wo_all, query, key, val, post, signal, conv_hid,
    attn_hid, hin, both,
    l_sem, z_send, z_recv, f_send, f_recv, g_send, g_recv, r_send, r_recv, t_send, t_recv,
    p_send, p_recv, o_send, o_recv, of_send, of_recv, og_send, og_recv, c_send, c_recv,
    a_send, a_recv, e_send, e_recv, s_sem,
):
    z, f, c = lax.axis_index("sp"), lax.axis_index("fs"), lax.axis_index("tp")
    beside, above = f + 1 - 2 * (f % 2), f + 2 - 4 * (f // 2)
    near = sorted(range(1, n), key=lambda d: min(d, n - d))
    fs = 2 * wo_all.shape[0] // n
    rows = tok_ref.shape[0]
    w_rows = q_ref.shape[0]
    total_rows = rows * n
    vsize = v_ref.shape[1] // n
    channels = post_ref.shape[1] // n
    wide = 2 * half
    o_attn = ao_ref.shape[1]
    bf16, f32 = jnp.bfloat16, jnp.float32

    members = ((q_ref, wide), (k_ref, wide), (pre_ref, channels), (inner_ref, channels),
               (post_ref, channels), (v_ref, vsize))
    starts = [0]
    for ref, width in members:
        starts.append(starts[-1] + width)

    def w_place(s, g):
        return w_all.at[pl.ds(pl.multiple_of((s * fs + g) * w_rows, w_rows), w_rows)]

    tok_load = load(tok_ref, t_raw, l_sem.at[n * 6])
    tok_load.start()
    loads = {}
    for d in near + [0]:
        to = (z + d) % n
        target = pack.at[d] if d else w_place(z, f)
        loads[d] = []
        for m, (ref, width) in enumerate(members):
            piece = load(
                ref.at[:, pl.ds(pl.multiple_of(to * width, width), width)],
                target.at[:, pl.ds(starts[m], width)],
                l_sem.at[d * 6 + m],
            )
            piece.start()
            loads[d].append(piece)
    o_loads = [
        load(ao_ref, o_raw.at[:, pl.ds(0, o_attn)], l_sem.at[n * 6 + 1]),
        load(co_ref, o_raw.at[:, pl.ds(o_attn, co_ref.shape[1])], l_sem.at[n * 6 + 2]),
    ]
    place = c * n + z
    small = [
        load(source, target, l_sem.at[n * 6 + 3 + at])
        for at, (source, target) in enumerate((
            (ng_any, gain_ref), (qg_any, qg_ref), (kg_any, kg_ref), (hg_any, hg_ref),
            (taps_any.at[:, pl.ds(pl.multiple_of(place * channels, channels), channels)], taps_ref),
        ))
    ]
    for piece in o_loads + small:
        piece.start()

    meet([{"sp": (z + d) % n} for d in near] + [{"fs": beside}, {"fs": above}, {"tp": 1 - c}])

    flights = []

    def go(copy):
        copy.start()
        flights.append(copy)
        return copy

    tok_load.wait()
    raw = go(remote(t_raw, t_twin, r_send.at[0], r_recv.at[0], {"tp": 1 - c}))
    across = {}
    for d in near:
        for piece in loads[d]:
            piece.wait()
        across[d] = go(
            remote(pack.at[d], w_place(z, f), z_send.at[d], z_recv.at[d], {"sp": (z + d) % n})
        )
    for piece in loads[0]:
        piece.wait()
    side = {}

    def spread(d):
        s = (z + n - d) % n
        for i, to in enumerate((beside, above)):
            side[i, d] = go(
                remote(w_place(s, f), w_place(s, f), f_send.at[i, d], f_recv.at[i, d], {"fs": to})
            )

    further = {}

    def pass_on(d):
        s = (z + n - d) % n
        i = d % 2
        side[i, d].wait_recv()
        held, to = (beside, above) if i == 0 else (above, beside)
        further[d] = go(
            remote(w_place(s, held), w_place(s, held), g_send.at[d], g_recv.at[d], {"fs": to})
        )

    spread(0)

    for piece in small:
        piece.wait()
    raw.wait_recv()
    tile = math.gcd(rows, 64)

    def norm_rows(i, unused):
        at = pl.ds(pl.multiple_of(i * tile, tile), tile)
        to = pl.ds(pl.multiple_of(z * rows + i * tile, tile), tile)
        own, twin = t_raw[at, :].astype(f32), t_twin[at, :].astype(f32)
        square = jnp.sum(own * own, axis=-1, keepdims=True) + jnp.sum(
            twin * twin, axis=-1, keepdims=True
        )
        factor = lax.rsqrt(square / (2 * own.shape[1]) + epsilon)
        t_all[c, to, :] = (own * factor * gain_ref[c]).astype(bf16)
        t_all[1 - c, to, :] = (twin * factor * gain_ref[1 - c]).astype(bf16)
        return unused

    lax.fori_loop(0, rows // tile, norm_rows, 0)

    def t_place(s):
        return t_all.at[c, pl.ds(pl.multiple_of(s * rows, rows), rows)]

    def t_along(s, step):
        return remote(
            t_place(s), t_place(s), t_send.at[(step + 1) // 2, s], t_recv.at[s], {"sp": z + step}
        )

    def t_aside(s):
        return remote(t_place(s), t_place(s), p_send.at[s], p_recv.at[s], {"tp": 1 - c})

    def o_place(s, g):
        at = s * fs + g
        return wo_all.at[at // 2, :, pl.ds(pl.multiple_of(at % 2 * w_rows, w_rows), w_rows)]

    def o_along(s, step):
        return remote(
            o_place(s, f), o_place(s, f), o_send.at[(step + 1) // 2, s], o_recv.at[s],
            {"sp": z + step},
        )

    def o_side(s, i):
        return remote(
            o_place(s, f), o_place(s, f), of_send.at[i, s], of_recv.at[i, s],
            {"fs": (beside, above)[i]},
        )

    def o_further(s, d):
        held, to = (beside, above) if d % 2 == 0 else (above, beside)
        return remote(
            o_place(s, held), o_place(s, held), og_send.at[s], og_recv.at[s], {"fs": to}
        )

    def both_ways(along):
        for step in (1, -1):
            @pl.when(jnp.logical_and(z + step >= 0, z + step < n))
            def _(step=step):
                along(z, step).start()

    both_ways(t_along)

    for piece in o_loads:
        piece.wait()
    square = o_raw.shape[0]
    for i in range(o_raw.shape[1] // square):
        wo_all[
            (z * fs + f) // 2, i * square:(i + 1) * square,
            pl.ds(pl.multiple_of(f % 2 * w_rows, w_rows), w_rows),
        ] = o_raw[:, i * square:(i + 1) * square].T
    both_ways(o_along)

    last = 0
    for d in near:
        across[d].wait_recv()
        spread(d)
        pass_on(last)
        last = d
    pass_on(last)
    for i in range(2):
        o_side(z, i).start()
    for d in range(n):
        side[1 - d % 2, d].wait_recv()
        further[d].wait_recv()

    order = [sorted(range(n), key=lambda s: (abs(s - at), s > at if 2 * at < n else s < at))
             for at in range(n)]

    def t_event(at, s):
        t_along(s, 1).wait_recv()
        step = 1 if s < at else -1
        if 0 <= at + step < n:
            t_along(s, step).start()
        t_aside(s).start()

    def o_event(at, s):
        o_along(s, 1).wait_recv()
        step = 1 if s < at else -1
        if 0 <= at + step < n:
            o_along(s, step).start()
        for i in range(2):
            o_side(s, i).start()

    def o_pass(at, s):
        d = (at - s) % n
        o_side(s, d % 2).wait_recv()
        o_further(s, d).start()

    plans = []
    for at in range(n):
        plan, t_done, o_done, passed = [], {at}, [at], []
        for visit in range(1, n):
            events, held = [], [r for r in o_done if r not in passed]
            s = order[at][visit]
            if s not in t_done:
                ring = [r for r in order[at] if abs(r - at) == abs(s - at)]
                events += [(t_event, r) for r in ring]
                t_done |= set(ring)
                if visit + len(ring) < n:
                    events += [(o_event, r) for r in ring]
                    o_done += ring
            plan.append(events + [(o_pass, r) for r in held])
            passed += held
        plan.append([(o_event, r) for r in order[at] if r not in o_done])
        plan.append([(o_pass, r) for r in order[at] if r not in passed])
        plans.append(plan)

    def follow(events):
        for at in range(n):
            if events(at):
                @pl.when(z == at)
                def _(at=at):
                    for event, s in events(at):
                        event(at, s)

    deep = t_all.shape[2]
    m_rows = math.gcd(rows, 256)

    q_gain = jnp.concatenate([qg_ref[...], qg_ref[...]], axis=1)
    k_gain = jnp.concatenate([kg_ref[...], kg_ref[...]], axis=1)

    def project(s):
        def some(i, unused):
            base = pl.multiple_of(s * rows + i * m_rows, m_rows)
            at = pl.ds(base, m_rows)

            def product(first, final):
                lo, hi = starts[first], starts[final]
                return jnp.dot(
                    t_all[0, at, :], w_all[0:deep, lo:hi], preferred_element_type=f32
                ) + jnp.dot(
                    t_all[1, at, :], w_all[deep:2 * deep, lo:hi], preferred_element_type=f32
                )

            pair = product(0, 2)
            low = lax.broadcasted_iota(jnp.int32, (1, wide), 1) < half
            q = half_scaled(pair[:, :wide], q_gain, half).astype(bf16).astype(f32)
            query[0, at, :] = jnp.where(low, q, 0.0).astype(bf16)
            query[1, at, :] = jnp.where(low, 0.0, q).astype(bf16)
            key[at, :] = half_scaled(pair[:, wide:], k_gain, half).astype(bf16)
            mixed = product(2, 3) * product(3, 4)
            signal[pl.ds(base + 8, m_rows), :] = mixed.astype(bf16).astype(f32)
            post[at, :] = product(4, 5).astype(bf16)
            val[at, :] = product(5, 6).astype(bf16)
            return unused

        lax.fori_loop(0, rows // m_rows, some, 0)

    signal[0:8, :] = jnp.zeros((8, channels), f32)
    signal[total_rows + 8:total_rows + 16, :] = jnp.zeros((8, channels), f32)
    h_rows = math.gcd(rows, 64)
    conv_at = pl.ds(pl.multiple_of(o_attn + z * channels, channels), channels)
    attn_at = pl.ds(pl.multiple_of(z * vsize, vsize), vsize)
    own = pl.ds(pl.multiple_of(z * rows, rows), rows)

    def convolve(s):
        def some(i, unused):
            base = pl.multiple_of(s * rows + i * h_rows, h_rows)
            around = signal[pl.ds(base, h_rows + 16), :]
            filtered = (
                taps_ref[0:1] * around[7:7 + h_rows]
                + taps_ref[1:2] * around[8:8 + h_rows]
                + taps_ref[2:3] * around[9:9 + h_rows]
            )
            at = pl.ds(base, h_rows)
            conv_hid[at, :] = (post[at, :].astype(f32) * filtered).astype(bf16)
            return unused

        lax.fori_loop(0, rows // h_rows, some, 0)

    def sent_to(source, columns, to, send, recv):
        return remote(
            source.at[pl.ds(pl.multiple_of(to * rows, rows), rows)], hin.at[:, columns],
            send.at[to], recv.at[z], {"sp": to},
        )

    def c_copy(to):
        return sent_to(conv_hid, conv_at, to, c_send, c_recv)

    def a_copy(to):
        return sent_to(attn_hid, attn_at, to, a_send, a_recv)

    def convolve_send(s):
        @pl.when(s != z)
        def _():
            c_copy(s).start()

    whole = []
    for at in range(n):
        seen, out, stages = {at}, set(), []
        for visit in range(1, n):
            seen.add(order[at][visit])
            fresh = [r for r in order[at] if r not in out
                     and all(q in seen for q in (r - 1, r, r + 1) if 0 <= q < n)]
            out |= set(fresh)
            stages.append(fresh)
        whole.append(stages)
    counts = [max(len(whole[at][v]) for at in range(n)) for v in range(n - 1)]

    def each_whole(visit, act):
        for k in range(counts[visit - 1]):
            held = [whole[at][visit - 1] for at in range(n)]
            s = choose([p[k] if k < len(p) else -1 for p in held], z)
            if all(k < len(p) for p in held):
                act(s)
            else:
                @pl.when(s >= 0)
                def _(s=s):
                    act(s)

    project(z)
    for visit in range(1, n):
        follow(lambda at: plans[at][visit - 1])
        s = choose([order[at][visit] for at in range(n)], z)
        t_aside(s).wait_recv()
        project(s)
        each_whole(visit, convolve)
        each_whole(visit, convolve_send)
    hin[:, conv_at] = conv_hid[own, :]
    far = near[::-1]

    a_rows = math.gcd(rows, 256)
    each = rows // a_rows
    scale = half ** (-0.5) * math.log2(math.e)
    lam = lam_ref[place]

    def attend(i, unused):
        for k, when in enumerate((0, (n * each) // 2 + 1)):
            @pl.when(i == when)
            def _(k=k):
                follow(lambda at: plans[at][n - 1 + k])

        d = choose(far + [0], i // each)
        at = pl.ds(pl.multiple_of(((z + d) % n) * rows + (i % each) * a_rows, a_rows), a_rows)
        maps = []
        for which in range(2):
            scores = lax.dot_general(
                query[which, at, :], key[...], (((1,), (1,)), ((), ())),
                preferred_element_type=f32,
            ) * scale
            expo = jnp.exp2(scores - jnp.max(scores, axis=-1, keepdims=True))
            total = jnp.sum(expo, axis=-1, keepdims=True)
            maps.append(
                jnp.dot(expo.astype(bf16), val[...], preferred_element_type=f32) / total
            )
        head_out = maps[0] - lam * maps[1]
        attn_hid[at, :] = scale_rows(head_out, hg_ref[...]).astype(bf16)
        for j, d in enumerate(far):
            @pl.when(i == (j + 1) * each - 1)
            def _(d=d):
                a_copy((z + d) % n).start()
        return unused

    lax.fori_loop(0, n * each, attend, 0)
    hin[:, attn_at] = attn_hid[own, :]

    def arrived(source, columns, d, send, recv):
        s = (z + d) % n
        remote(
            source.at[pl.ds(0, rows)], hin.at[:, columns], send.at[s], recv.at[s], {"sp": s}
        ).wait_recv()

    for d in near:
        arrived(conv_hid, conv_at, d, c_send, c_recv)

    pairs = wo_all.shape[0]
    half_rows = rows // 2
    width = 2 * w_rows

    theirs = pl.ds(pl.multiple_of((1 - c) * half_rows, half_rows), half_rows)
    ours = pl.ds(pl.multiple_of(c * half_rows, half_rows), half_rows)

    def swap(j):
        at = pl.ds(pl.multiple_of(j * width, width), width)
        return remote(
            both.at[j, theirs], take.at[:, at], e_send.at[j], e_recv.at[j], {"tp": 1 - c}
        )

    def store(j):
        at = pl.ds(pl.multiple_of(j * width, width), width)
        return load(both.at[j, ours], mine.at[:, at], s_sem.at[j])

    def channel_part(j, unused):
        acc[j] = jnp.dot(hin[:, o_attn:], wo_all[j, o_attn:, :], preferred_element_type=f32)
        return unused

    for visit in range(n):
        s = choose([order[at][visit] for at in range(n)], z)
        for i in range(2):
            @pl.when((z + n - s) % 2 != i)
            def _(s=s, i=i):
                o_side(s, i).wait_recv()
        o_further(s, 0).wait_recv()
        lax.fori_loop(s * (fs // 2), (s + 1) * (fs // 2), channel_part, 0)
    for d in near:
        arrived(attn_hid, attn_at, d, a_send, a_recv)

    def head_part(j, unused):
        both[j] = (
            acc[j]
            + jnp.dot(hin[:, :o_attn], wo_all[j, :o_attn, :], preferred_element_type=f32)
        ).astype(bf16)
        swap(j).start()
        store(j).start()
        return unused

    lax.fori_loop(0, pairs, head_part, 0)
    for j in range(pairs):
        swap(j).wait_recv()
        store(j).wait()

    for copy in flights:
        copy.wait_send()
    for d in far:
        c_copy((z + d) % n).wait_send()
        a_copy((z + d) % n).wait_send()
    for j in range(pairs):
        swap(j).wait_send()
    for s in range(n):
        for i in range(2):
            o_side(s, i).wait_send()
        o_further(s, 0).wait_send()
        for step in (1, -1):
            arrives = s <= z if step == 1 else s >= z
            @pl.when(jnp.logical_and(arrives, jnp.logical_and(z + step >= 0, z + step < n)))
            def _(s=s, step=step):
                t_along(s, step).wait_send()
                o_along(s, step).wait_send()

        @pl.when(z != s)
        def _(s=s):
            t_aside(s).wait_send()


def split_device(
    inputs,
    norm_gain,
    query_weight,
    key_weight,
    value_weight,
    query_gain,
    key_gain,
    mix_lambda,
    head_gain,
    post_gate_weight,
    pre_gate_weight,
    inner_weight,
    conv_taps,
    attn_out_weight,
    conv_out_weight,
):
    n, fs, tp = lax.axis_size("sp"), lax.axis_size("fs"), lax.axis_size("tp")
    tokens = inputs[0]
    rows, deep = tokens.shape
    half, vsize = query_gain.shape[0], head_gain.shape[0]
    channels = post_gate_weight.shape[1] // n
    w_rows = query_weight.shape[0]
    columns = 4 * half + vsize + 3 * channels
    hidden = n * (vsize + channels)
    total = n * rows
    out_width = w_rows * n * fs
    pairs = n * fs // 2
    bf16, dma = jnp.bfloat16, pltpu.SemaphoreType.DMA
    far = pl.BlockSpec(memory_space=pl.ANY)
    mine, take = pl.pallas_call(
        lambda *refs: fused_kernel(n, half, *refs),
        out_shape=(jax.ShapeDtypeStruct((rows // tp, out_width), bf16),) * 2,
        in_specs=[far] * 12 + [pl.BlockSpec(memory_space=pltpu.SMEM)] + [far] * 2,
        out_specs=(far, far),
        scratch_shapes=[
            pltpu.VMEM((tp, 1, deep), jnp.float32),
            pltpu.VMEM((1, half), jnp.float32),
            pltpu.VMEM((1, half), jnp.float32),
            pltpu.VMEM((1, vsize), jnp.float32),
            pltpu.VMEM((3, channels), jnp.float32),
            pltpu.VMEM((pairs, rows, 2 * w_rows), jnp.float32),
            pltpu.VMEM((n, w_rows, columns), bf16),
            pltpu.VMEM((n * fs * w_rows, columns), bf16),
            pltpu.VMEM((rows, deep), bf16),
            pltpu.VMEM((rows, deep), bf16),
            pltpu.VMEM((tp, total, deep), bf16),
            pltpu.VMEM((w_rows, hidden), bf16),
            pltpu.VMEM((pairs, hidden, 2 * w_rows), bf16),
            pltpu.VMEM((2, total, 2 * half), bf16),
            pltpu.VMEM((total, 2 * half), bf16),
            pltpu.VMEM((total, vsize), bf16),
            pltpu.VMEM((total, channels), bf16),
            pltpu.VMEM((total + 16, channels), jnp.float32),
            pltpu.VMEM((total, channels), bf16),
            pltpu.VMEM((total, vsize), bf16),
            pltpu.VMEM((rows, hidden), bf16),
            pltpu.VMEM((pairs, rows, 2 * w_rows), bf16),
            dma((n * 6 + 8,)),
            dma((n,)), dma((n,)), dma((2, n)), dma((2, n)), dma((n,)), dma((n,)),
            dma((1,)), dma((1,)), dma((2, n)), dma((n,)), dma((n,)), dma((n,)),
            dma((2, n)), dma((n,)), dma((2, n)), dma((2, n)), dma((n,)), dma((n,)),
            dma((n,)), dma((n,)), dma((n,)), dma((n,)), dma((pairs,)), dma((pairs,)), dma((pairs,)),
        ],
        compiler_params=pltpu.CompilerParams(
            collective_id=1, has_side_effects=True, vmem_limit_bytes=60 * 2**20
        ),
    )(
        tokens, query_weight, key_weight, value_weight, post_gate_weight, pre_gate_weight,
        inner_weight, attn_out_weight, conv_out_weight,
        norm_gain.reshape(tp, 1, deep),
        query_gain[None],
        key_gain[None],
        mix_lambda,
        head_gain[None],
        conv_taps,
    )
    return (mine.astype(jnp.float32) + take.astype(jnp.float32)).astype(bf16)[None]


def per_device(
    inputs,
    norm_gain,
    query_weight,
    key_weight,
    value_weight,
    query_gain,
    key_gain,
    mix_lambda,
    head_gain,
    post_gate_weight,
    pre_gate_weight,
    inner_weight,
    conv_taps,
    attn_out_weight,
    conv_out_weight,
):
    tokens = inputs[0]
    whole = lax.all_gather(tokens, "tp", axis=1, tiled=True)
    normed = scale_rows(whole.astype(jnp.float32), norm_gain).astype(jnp.bfloat16)
    heads_dev = value_weight.shape[1] // head_gain.shape[0]
    channels = post_gate_weight.shape[1]
    tp_index = lax.axis_index("tp")
    weight_two = lax.dynamic_slice_in_dim(mix_lambda, tp_index * heads_dev, heads_dev)
    taps = lax.dynamic_slice_in_dim(conv_taps, tp_index * channels, channels, 1)
    every_full = (
        lax.all_gather(query_weight, ("sp", "fs"), axis=0, tiled=True),
        lax.all_gather(key_weight, ("sp", "fs"), axis=0, tiled=True),
        lax.all_gather(value_weight, ("sp", "fs"), axis=0, tiled=True),
        lax.all_gather(post_gate_weight, ("sp", "fs"), axis=0, tiled=True),
        lax.all_gather(pre_gate_weight, ("sp", "fs"), axis=0, tiled=True),
        lax.all_gather(inner_weight, ("sp", "fs"), axis=0, tiled=True),
        lax.all_gather(attn_out_weight, ("sp", "fs"), axis=0, tiled=True),
        lax.all_gather(conv_out_weight, ("sp", "fs"), axis=0, tiled=True),
    )
    query, key, value_proj, post, pre_gate, inner, attn_out_full, conv_out_full = project_all(
        normed, every_full[0:3] + every_full[3:6] + every_full[6:8], 6
    )
    attn_hidden = attention_branch(
        query, key, value_proj.astype(jnp.bfloat16), weight_two, query_gain, key_gain, head_gain
    )
    post_mid = post.astype(jnp.bfloat16)
    post_wide = lax.optimization_barrier(post_mid).astype(jnp.float32)
    signal = (pre_gate * inner).astype(jnp.bfloat16)
    padded = padded_2(signal, (("sp", 0),), 1)
    shifted = lax.optimization_barrier(padded).astype(jnp.float32)
    filtered = taps[0] * shifted[:-2] + taps[1] * shifted[1:-1] + taps[2] * shifted[2:]
    conv_hidden = (post_wide * filtered).astype(jnp.bfloat16)
    contract = (((1,), (1,)), ((), ()))
    summed = lax.psum_scatter(
        (
            lax.dot_general(
                attn_hidden, attn_out_full, contract, preferred_element_type=jnp.float32
            )
            + lax.dot_general(
                conv_hidden, conv_out_full, contract, preferred_element_type=jnp.float32
            )
        ).astype(jnp.bfloat16),
        "tp",
        scatter_dimension=0,
        tiled=True,
    )
    return summed[None]


def solution(mesh):
    placed = (
        P("fs", "sp", "tp"),
        P(),
        P(("sp", "fs"), "tp"),
        P(("sp", "fs"), "tp"),
        P(("sp", "fs"), "tp"),
        P(),
        P(),
        P(),
        P(),
        P(("sp", "fs"), "tp"),
        P(("sp", "fs"), "tp"),
        P(("sp", "fs"), "tp"),
        P(),
        P(("sp", "fs"), "tp"),
        P(("sp", "fs"), "tp"),
    )
    sp, tp = mesh.shape["sp"], mesh.shape["tp"]

    def program(*args):
        heads = args[7].shape[0]
        channels = args[12].shape[1]
        splits = tp == 2 and mesh.shape["fs"] == 4 and sp > 1 and heads == sp * tp
        splits = splits and channels % (sp * tp * 128) == 0
        return shard(split_device if splits else per_device)(*args)

    shard = lambda body: jax.shard_map(
        body,
        mesh=mesh,
        in_specs=placed,
        out_specs=P("fs", ("sp", "tp"), None),
        check_vma=False,
    )

    return program
```

```python
import math

import jax
import jax.numpy as jnp
from jax import lax
from jax.experimental import pallas as pl
from jax.experimental.pallas import tpu as pltpu
from jax.sharding import PartitionSpec as P

epsilon = 1e-06


def padded_2(x, sides, width):
    for axis, dim in sides:
        size, length = (lax.axis_size(axis), x.shape[dim])
        up = [(i, (i + 1) % size) for i in range(size - 1)]
        down = [(j, i) for i, j in up]
        last = lax.slice_in_dim(x, length - width, length, axis=dim)
        initial = lax.slice_in_dim(x, 0, width, axis=dim)
        before = lax.ppermute(last, axis, up)
        after = lax.ppermute(initial, axis, down)
        x = jnp.concatenate([before, x, after], axis=dim)
    return x


def scale_rows(values, gain):
    return values * lax.rsqrt(jnp.mean(values * values, axis=-1, keepdims=True) + epsilon) * gain


def project_all(normed, weights, products):
    result = []
    for member in range(len(weights)):
        if member < products:
            result.append(jnp.dot(normed, weights[member], preferred_element_type=jnp.float32))
        else:
            result.append(weights[member])
    return tuple(result)


def attention_branch(query, key, values, weight_two, query_gain, key_gain, head_gain):
    tok_rows = query.shape[0]
    vsize = head_gain.shape[0]
    half = query_gain.shape[0]
    heads = values.shape[1] // vsize
    query_normed = scale_rows(query.reshape(tok_rows, heads, 2, half), query_gain).astype(
        jnp.bfloat16
    )
    key_normed = scale_rows(key.reshape(tok_rows, heads * 2, half), key_gain).astype(jnp.bfloat16)
    key_normed = key_normed.reshape(tok_rows, heads * 2 * half)
    scale = half ** (-0.5)
    initial = (
        jnp.full((heads, 2, tok_rows), -1e30, jnp.float32),
        jnp.zeros((heads, 2, tok_rows), jnp.float32),
        jnp.zeros((heads, 2, tok_rows, vsize), jnp.float32),
    )
    carry = initial
    key_piece = lax.all_gather(key_normed, "sp", axis=0, tiled=True)
    value_piece = lax.all_gather(values, "sp", axis=0, tiled=True)
    length = key_piece.shape[0]
    block = math.gcd(length, 512)
    key_blocks = key_piece.reshape(length // block, block, heads, 2, half)
    value_blocks = value_piece.reshape(length // block, block, heads, vsize)

    def one_block(state, blocks):
        peak, total, accum = state
        key_block, value_block = blocks
        scores = (
            jnp.einsum(
                "qhjd,khjd->hjqk", query_normed, key_block, preferred_element_type=jnp.float32
            )
            * scale
        )
        new_peak = jnp.maximum(peak, jnp.max(scores, axis=-1))
        factor = jnp.exp(peak - new_peak)
        expo = jnp.exp(scores - new_peak[..., None])
        total = total * factor + jnp.sum(expo, axis=-1)
        accum = accum * factor[..., None] + jnp.einsum(
            "hjqk,khd->hjqd",
            expo.astype(jnp.bfloat16),
            value_block,
            preferred_element_type=jnp.float32,
        )
        return ((new_peak, total, accum), None)

    carry, unused = lax.scan(one_block, carry, (key_blocks, value_blocks))
    peak, total, accum = carry
    mapped = accum / total[..., None]
    head_out = mapped[:, 0] - weight_two[:, None, None] * mapped[:, 1]
    normed_out = scale_rows(head_out, head_gain).astype(jnp.bfloat16)
    return jnp.transpose(normed_out, (1, 0, 2)).reshape(tok_rows, heads * vsize)


def half_scaled(values, gain, half):
    low = lax.broadcasted_iota(jnp.int32, (1, 2 * half), 1) < half
    squares = values * values
    first = jnp.sum(jnp.where(low, squares, 0.0), axis=-1, keepdims=True) / half
    second = jnp.sum(jnp.where(low, 0.0, squares), axis=-1, keepdims=True) / half
    factor = jnp.where(low, lax.rsqrt(first + epsilon), lax.rsqrt(second + epsilon))
    return values * factor * gain


def remote(source, target, send, recv, where):
    return pltpu.make_async_remote_copy(
        src_ref=source,
        dst_ref=target,
        send_sem=send,
        recv_sem=recv,
        device_id=where,
        device_id_type=pl.DeviceIdType.MESH,
    )


def meet(places):
    barrier = pltpu.get_barrier_semaphore()
    for where in places:
        pl.semaphore_signal(
            barrier, inc=1, device_id=where, device_id_type=pl.DeviceIdType.MESH
        )
    pl.semaphore_wait(barrier, len(places))


def load(source, target, sem):
    return pltpu.make_async_copy(source, target, sem)


def choose(table, z):
    value = table[0]
    for at in range(1, len(table)):
        value = jnp.where(z == at, table[at], value)
    return value


def fused_kernel(
    n, half, tok_ref, q_ref, k_ref, v_ref, post_ref, pre_ref, inner_ref, ao_ref, co_ref,
    ng_any, qg_any, kg_any, lam_ref, hg_any, taps_any, mine, take,
    gain_ref, qg_ref, kg_ref, hg_ref, taps_ref, acc, pack, w_all, t_raw, t_twin, t_all, o_raw, wo_all, query, key, val, post, signal, conv_hid,
    attn_hid, hin, both, part_peak, part_total, part_sum,
    l_sem, z_send, z_recv, f_send, f_recv, g_send, g_recv, r_send, r_recv, t_send, t_recv,
    p_send, p_recv, o_send, o_recv, of_send, of_recv, og_send, og_recv, c_send, c_recv,
    a_send, a_recv, e_send, e_recv, s_sem,
):
    z, f, c = lax.axis_index("sp"), lax.axis_index("fs"), lax.axis_index("tp")
    beside, above = f + 1 - 2 * (f % 2), f + 2 - 4 * (f // 2)
    near = sorted(range(1, n), key=lambda d: min(d, n - d))
    fs = 2 * wo_all.shape[0] // n
    rows = tok_ref.shape[0]
    w_rows = q_ref.shape[0]
    total_rows = rows * n
    vsize = v_ref.shape[1] // n
    channels = post_ref.shape[1] // n
    wide = 2 * half
    o_attn = ao_ref.shape[1]
    bf16, f32 = jnp.bfloat16, jnp.float32

    members = ((q_ref, wide), (k_ref, wide), (pre_ref, channels), (inner_ref, channels),
               (post_ref, channels), (v_ref, vsize))
    starts = [0]
    for ref, width in members:
        starts.append(starts[-1] + width)

    def w_place(s, g):
        return w_all.at[pl.ds(pl.multiple_of((s * fs + g) * w_rows, w_rows), w_rows)]

    tok_load = load(tok_ref, t_raw, l_sem.at[n * 6])
    tok_load.start()
    loads = {}
    for d in near + [0]:
        to = (z + d) % n
        target = pack.at[d] if d else w_place(z, f)
        loads[d] = []
        for m, (ref, width) in enumerate(members):
            piece = load(
                ref.at[:, pl.ds(pl.multiple_of(to * width, width), width)],
                target.at[:, pl.ds(starts[m], width)],
                l_sem.at[d * 6 + m],
            )
            piece.start()
            loads[d].append(piece)
    o_loads = [
        load(ao_ref, o_raw.at[:, pl.ds(0, o_attn)], l_sem.at[n * 6 + 1]),
        load(co_ref, o_raw.at[:, pl.ds(o_attn, co_ref.shape[1])], l_sem.at[n * 6 + 2]),
    ]
    place = c * n + z
    small = [
        load(source, target, l_sem.at[n * 6 + 3 + at])
        for at, (source, target) in enumerate((
            (ng_any, gain_ref), (qg_any, qg_ref), (kg_any, kg_ref), (hg_any, hg_ref),
            (taps_any.at[:, pl.ds(pl.multiple_of(place * channels, channels), channels)], taps_ref),
        ))
    ]
    for piece in o_loads + small:
        piece.start()

    meet([{"sp": (z + d) % n} for d in near] + [{"fs": beside}, {"fs": above}, {"tp": 1 - c}])

    flights = []

    def go(copy):
        copy.start()
        flights.append(copy)
        return copy

    tok_load.wait()
    raw = go(remote(t_raw, t_twin, r_send.at[0], r_recv.at[0], {"tp": 1 - c}))
    across = {}
    for d in near:
        for piece in loads[d]:
            piece.wait()
        across[d] = go(
            remote(pack.at[d], w_place(z, f), z_send.at[d], z_recv.at[d], {"sp": (z + d) % n})
        )
    for piece in loads[0]:
        piece.wait()
    side = {}

    def spread(d):
        s = (z + n - d) % n
        for i, to in enumerate((beside, above)):
            side[i, d] = go(
                remote(w_place(s, f), w_place(s, f), f_send.at[i, d], f_recv.at[i, d], {"fs": to})
            )

    further = {}

    def pass_on(d):
        s = (z + n - d) % n
        i = d % 2
        side[i, d].wait_recv()
        held, to = (beside, above) if i == 0 else (above, beside)
        further[d] = go(
            remote(w_place(s, held), w_place(s, held), g_send.at[d], g_recv.at[d], {"fs": to})
        )

    spread(0)

    for piece in small:
        piece.wait()
    raw.wait_recv()
    tile = math.gcd(rows, 64)

    def norm_rows(i, unused):
        at = pl.ds(pl.multiple_of(i * tile, tile), tile)
        to = pl.ds(pl.multiple_of(z * rows + i * tile, tile), tile)
        own, twin = t_raw[at, :].astype(f32), t_twin[at, :].astype(f32)
        square = jnp.sum(own * own, axis=-1, keepdims=True) + jnp.sum(
            twin * twin, axis=-1, keepdims=True
        )
        factor = lax.rsqrt(square / (2 * own.shape[1]) + epsilon)
        t_all[c, to, :] = (own * factor * gain_ref[c]).astype(bf16)
        t_all[1 - c, to, :] = (twin * factor * gain_ref[1 - c]).astype(bf16)
        return unused

    lax.fori_loop(0, rows // tile, norm_rows, 0)

    def t_place(s):
        return t_all.at[c, pl.ds(pl.multiple_of(s * rows, rows), rows)]

    def t_along(s, step):
        return remote(
            t_place(s), t_place(s), t_send.at[(step + 1) // 2, s], t_recv.at[s], {"sp": z + step}
        )

    def t_aside(s):
        return remote(t_place(s), t_place(s), p_send.at[s], p_recv.at[s], {"tp": 1 - c})

    def o_place(s, g):
        at = s * fs + g
        return wo_all.at[at // 2, :, pl.ds(pl.multiple_of(at % 2 * w_rows, w_rows), w_rows)]

    def o_along(s, step):
        return remote(
            o_place(s, f), o_place(s, f), o_send.at[(step + 1) // 2, s], o_recv.at[s],
            {"sp": z + step},
        )

    def o_side(s, i):
        return remote(
            o_place(s, f), o_place(s, f), of_send.at[i, s], of_recv.at[i, s],
            {"fs": (beside, above)[i]},
        )

    def o_further(s, part):
        held, to = (beside, above) if part == 0 else (above, beside)
        at, size = s * fs + held, wo_all.shape[1] // 2
        block = wo_all.at[
            at // 2, pl.ds(part * size, size),
            pl.ds(pl.multiple_of(at % 2 * w_rows, w_rows), w_rows),
        ]
        return remote(block, block, og_send.at[part, s], og_recv.at[part, s], {"fs": to})

    def both_ways(along):
        for step in (1, -1):
            @pl.when(jnp.logical_and(z + step >= 0, z + step < n))
            def _(step=step):
                along(z, step).start()

    both_ways(t_along)

    for piece in o_loads:
        piece.wait()
    square = o_raw.shape[0]
    for i in range(o_raw.shape[1] // square):
        wo_all[
            (z * fs + f) // 2, i * square:(i + 1) * square,
            pl.ds(pl.multiple_of(f % 2 * w_rows, w_rows), w_rows),
        ] = o_raw[:, i * square:(i + 1) * square].T
    both_ways(o_along)

    last = 0
    for d in near:
        across[d].wait_recv()
        spread(d)
        pass_on(last)
        last = d
    pass_on(last)
    for i in range(2):
        o_side(z, i).start()
    for d in range(n):
        side[1 - d % 2, d].wait_recv()
        further[d].wait_recv()

    order = [sorted(range(n), key=lambda s: (abs(s - at), s > at if 2 * at < n else s < at))
             for at in range(n)]

    def t_event(at, s):
        t_along(s, 1).wait_recv()
        step = 1 if s < at else -1
        if 0 <= at + step < n:
            t_along(s, step).start()
        t_aside(s).start()

    def o_event(at, s):
        o_along(s, 1).wait_recv()
        step = 1 if s < at else -1
        if 0 <= at + step < n:
            o_along(s, step).start()
        for i in range(2):
            o_side(s, i).start()

    def o_pass(at, s):
        for part in range(2):
            o_side(s, part).wait_recv()
            o_further(s, part).start()

    plans = []
    for at in range(n):
        plan, t_done, o_done, passed = [], {at}, [at], []
        for visit in range(1, n):
            events, held = [], [r for r in o_done if r not in passed]
            s = order[at][visit]
            if s not in t_done:
                ring = [r for r in order[at] if abs(r - at) == abs(s - at)]
                events += [(t_event, r) for r in ring]
                t_done |= set(ring)
                if visit + len(ring) < n:
                    events += [(o_event, r) for r in ring]
                    o_done += ring
            passes = [(o_pass, r) for r in held]
            plan.append(passes + events if visit == n - 1 else events + passes)
            passed += held
        plan.append([(o_event, r) for r in order[at] if r not in o_done])
        plan.append([(o_pass, r) for r in order[at] if r not in passed])
        plans.append(plan)

    def follow(events):
        for at in range(n):
            if events(at):
                @pl.when(z == at)
                def _(at=at):
                    for event, s in events(at):
                        event(at, s)

    deep = t_all.shape[2]
    m_rows = math.gcd(rows, 256)

    q_gain = jnp.concatenate([qg_ref[...], qg_ref[...]], axis=1)
    k_gain = jnp.concatenate([kg_ref[...], kg_ref[...]], axis=1)

    def project(s):
        def some(i, unused):
            base = pl.multiple_of(s * rows + i * m_rows, m_rows)
            at = pl.ds(base, m_rows)

            def product(first, final):
                lo, hi = starts[first], starts[final]
                return jnp.dot(
                    t_all[0, at, :], w_all[0:deep, lo:hi], preferred_element_type=f32
                ) + jnp.dot(
                    t_all[1, at, :], w_all[deep:2 * deep, lo:hi], preferred_element_type=f32
                )

            pair = product(0, 2)
            low = lax.broadcasted_iota(jnp.int32, (1, wide), 1) < half
            q = half_scaled(pair[:, :wide], q_gain, half).astype(bf16).astype(f32)
            query[0, at, :] = jnp.where(low, q, 0.0).astype(bf16)
            query[1, at, :] = jnp.where(low, 0.0, q).astype(bf16)
            key[at, :] = half_scaled(pair[:, wide:], k_gain, half).astype(bf16)
            mixed = product(2, 3) * product(3, 4)
            signal[pl.ds(base + 8, m_rows), :] = mixed.astype(bf16).astype(f32)
            post[at, :] = product(4, 5).astype(bf16)
            val[at, :] = product(5, 6).astype(bf16)
            return unused

        lax.fori_loop(0, rows // m_rows, some, 0)

    signal[0:8, :] = jnp.zeros((8, channels), f32)
    signal[total_rows + 8:total_rows + 16, :] = jnp.zeros((8, channels), f32)
    h_rows = math.gcd(rows, 64)
    conv_at = pl.ds(pl.multiple_of(o_attn + z * channels, channels), channels)
    attn_at = pl.ds(pl.multiple_of(z * vsize, vsize), vsize)
    own = pl.ds(pl.multiple_of(z * rows, rows), rows)

    def convolve(s):
        def some(i, unused):
            base = pl.multiple_of(s * rows + i * h_rows, h_rows)
            around = signal[pl.ds(base, h_rows + 16), :]
            filtered = (
                taps_ref[0:1] * around[7:7 + h_rows]
                + taps_ref[1:2] * around[8:8 + h_rows]
                + taps_ref[2:3] * around[9:9 + h_rows]
            )
            at = pl.ds(base, h_rows)
            conv_hid[at, :] = (post[at, :].astype(f32) * filtered).astype(bf16)
            return unused

        lax.fori_loop(0, rows // h_rows, some, 0)

    def sent_to(source, columns, to, send, recv):
        return remote(
            source.at[pl.ds(pl.multiple_of(to * rows, rows), rows)], hin.at[:, columns],
            send.at[to], recv.at[z], {"sp": to},
        )

    def c_copy(to):
        return sent_to(conv_hid, conv_at, to, c_send, c_recv)

    def a_copy(to):
        return sent_to(attn_hid, attn_at, to, a_send, a_recv)

    def convolve_send(s):
        @pl.when(s != z)
        def _():
            c_copy(s).start()

    whole = []
    for at in range(n):
        seen, out, stages = {at}, set(), []
        for visit in range(1, n):
            seen.add(order[at][visit])
            fresh = [r for r in order[at] if r not in out
                     and all(q in seen for q in (r - 1, r, r + 1) if 0 <= q < n)]
            out |= set(fresh)
            stages.append(fresh)
        whole.append(stages)
    counts = [max(len(whole[at][v]) for at in range(n)) for v in range(n - 1)]

    def each_whole(visit, act):
        for k in range(counts[visit - 1]):
            held = [whole[at][visit - 1] for at in range(n)]
            s = choose([p[k] if k < len(p) else -1 for p in held], z)
            if all(k < len(p) for p in held):
                act(s)
            else:
                @pl.when(s >= 0)
                def _(s=s):
                    act(s)

    a_rows = math.gcd(rows, 256)
    each = rows // a_rows
    scale = half ** (-0.5) * math.log2(math.e)
    lam = lam_ref[place]
    is_end = jnp.logical_or(z == 0, z == n - 1)
    final = choose([order[at][n - 1] for at in range(n)], z)

    def compare(which, at, keys):
        return lax.dot_general(
            query[which, at, :], key[keys, :], (((1,), (1,)), ((), ())),
            preferred_element_type=f32,
        ) * scale

    def soft(which, at, keys):
        scores = compare(which, at, keys)
        peak = jnp.max(scores, axis=-1, keepdims=True)
        expo = jnp.exp2(scores - peak)
        total = jnp.sum(expo, axis=-1, keepdims=True)
        return peak, total, jnp.dot(
            expo.astype(bf16), val[keys, :], preferred_element_type=f32
        )

    def attend_first():
        start = jnp.where(final == 0, rows, 0)
        keys = pl.ds(pl.multiple_of(start, rows), total_rows - rows)

        def some(i, unused):
            at = pl.ds(pl.multiple_of(start + i * a_rows, a_rows), a_rows)
            for which in range(2):
                peak, total, accum = soft(which, at, keys)
                part_peak[which, at, :] = peak
                part_total[which, at, :] = total
                part_sum[which, at, :] = accum
            return unused

        lax.fori_loop(0, (n - 1) * each, some, 0)

    project(z)
    for visit in range(1, n):
        if visit == n - 1:
            pl.when(is_end)(attend_first)
        follow(lambda at: plans[at][visit - 1])
        s = choose([order[at][visit] for at in range(n)], z)
        t_aside(s).wait_recv()
        project(s)
        each_whole(visit, convolve)

        @pl.when(is_end)
        def _(visit=visit):
            each_whole(visit, convolve_send)
    hin[:, conv_at] = conv_hid[own, :]
    pl.when(jnp.logical_not(is_end))(attend_first)
    far = near[::-1]

    follow_rest = [lambda at, k=k: plans[at][n - 1 + k] for k in range(2)]

    def attend(i, unused):
        @pl.when(i == jnp.where(is_end, (n * each) // 2, 0))
        def _():
            follow(follow_rest[0])

            @pl.when(jnp.logical_not(is_end))
            def _():
                for visit in range(1, n):
                    each_whole(visit, convolve_send)

        @pl.when(jnp.logical_and(i == n * each - 2, jnp.logical_not(is_end)))
        def _():
            follow(follow_rest[1])

        block = (z + choose(far + [0], i // each)) % n
        at = pl.ds(pl.multiple_of(block * rows + (i % each) * a_rows, a_rows), a_rows)

        def finish(maps):
            head_out = maps[0] - lam * maps[1]
            attn_hid[at, :] = scale_rows(head_out, hg_ref[...]).astype(bf16)

        @pl.when(block != final)
        def _():
            maps = []
            late = pl.ds(pl.multiple_of(final * rows, rows), rows)
            for which in range(2):
                scores = compare(which, at, late)
                before = part_peak[which, at, :]
                peak = jnp.maximum(before, jnp.max(scores, axis=-1, keepdims=True))
                factor, expo = jnp.exp2(before - peak), jnp.exp2(scores - peak)
                total = part_total[which, at, :] * factor + jnp.sum(expo, axis=-1, keepdims=True)
                accum = part_sum[which, at, :] * factor + jnp.dot(
                    expo.astype(bf16), val[late, :], preferred_element_type=f32
                )
                maps.append(accum / total)
            finish(maps)

        @pl.when(block == final)
        def _():
            maps = []
            for which in range(2):
                unused_peak, total, accum = soft(which, at, pl.ds(0, total_rows))
                maps.append(accum / total)
            finish(maps)

        for j, d in enumerate(far):
            @pl.when(i == (j + 1) * each - 1)
            def _(d=d):
                a_copy((z + d) % n).start()
        return unused

    lax.fori_loop(0, n * each, attend, 0)

    @pl.when(is_end)
    def _():
        follow(follow_rest[1])

    hin[:, attn_at] = attn_hid[own, :]

    def arrived(source, columns, d, send, recv):
        s = (z + d) % n
        remote(
            source.at[pl.ds(0, rows)], hin.at[:, columns], send.at[s], recv.at[s], {"sp": s}
        ).wait_recv()

    for d in near:
        arrived(conv_hid, conv_at, d, c_send, c_recv)

    pairs = wo_all.shape[0]
    half_rows = rows // 2
    width = 2 * w_rows

    theirs = pl.ds(pl.multiple_of((1 - c) * half_rows, half_rows), half_rows)
    ours = pl.ds(pl.multiple_of(c * half_rows, half_rows), half_rows)

    def swap(j):
        at = pl.ds(pl.multiple_of(j * width, width), width)
        return remote(
            both.at[j, theirs], take.at[:, at], e_send.at[j], e_recv.at[j], {"tp": 1 - c}
        )

    def store(j):
        at = pl.ds(pl.multiple_of(j * width, width), width)
        return load(both.at[j, ours], mine.at[:, at], s_sem.at[j])

    def channel_part(j, unused):
        acc[j] = jnp.dot(hin[:, o_attn:], wo_all[j, o_attn:, :], preferred_element_type=f32)
        return unused

    for visit in range(n):
        s = choose([order[at][visit] for at in range(n)], z)
        for part in range(2):
            o_further(s, part).wait_recv()
        lax.fori_loop(s * (fs // 2), (s + 1) * (fs // 2), channel_part, 0)
    for d in near:
        arrived(attn_hid, attn_at, d, a_send, a_recv)

    def head_part(j, unused):
        both[j] = (
            acc[j]
            + jnp.dot(hin[:, :o_attn], wo_all[j, :o_attn, :], preferred_element_type=f32)
        ).astype(bf16)
        swap(j).start()
        store(j).start()
        return unused

    lax.fori_loop(0, pairs, head_part, 0)
    for j in range(pairs):
        swap(j).wait_recv()
        store(j).wait()

    for copy in flights:
        copy.wait_send()
    for d in far:
        c_copy((z + d) % n).wait_send()
        a_copy((z + d) % n).wait_send()
    for j in range(pairs):
        swap(j).wait_send()
    for s in range(n):
        for i in range(2):
            o_side(s, i).wait_send()
            o_further(s, i).wait_send()
        for step in (1, -1):
            arrives = s <= z if step == 1 else s >= z
            @pl.when(jnp.logical_and(arrives, jnp.logical_and(z + step >= 0, z + step < n)))
            def _(s=s, step=step):
                t_along(s, step).wait_send()
                o_along(s, step).wait_send()

        @pl.when(z != s)
        def _(s=s):
            t_aside(s).wait_send()


def split_device(
    inputs,
    norm_gain,
    query_weight,
    key_weight,
    value_weight,
    query_gain,
    key_gain,
    mix_lambda,
    head_gain,
    post_gate_weight,
    pre_gate_weight,
    inner_weight,
    conv_taps,
    attn_out_weight,
    conv_out_weight,
):
    n, fs, tp = lax.axis_size("sp"), lax.axis_size("fs"), lax.axis_size("tp")
    tokens = inputs[0]
    rows, deep = tokens.shape
    half, vsize = query_gain.shape[0], head_gain.shape[0]
    channels = post_gate_weight.shape[1] // n
    w_rows = query_weight.shape[0]
    columns = 4 * half + vsize + 3 * channels
    hidden = n * (vsize + channels)
    total = n * rows
    out_width = w_rows * n * fs
    pairs = n * fs // 2
    bf16, dma = jnp.bfloat16, pltpu.SemaphoreType.DMA
    far = pl.BlockSpec(memory_space=pl.ANY)
    mine, take = pl.pallas_call(
        lambda *refs: fused_kernel(n, half, *refs),
        out_shape=(jax.ShapeDtypeStruct((rows // tp, out_width), bf16),) * 2,
        in_specs=[far] * 12 + [pl.BlockSpec(memory_space=pltpu.SMEM)] + [far] * 2,
        out_specs=(far, far),
        scratch_shapes=[
            pltpu.VMEM((tp, 1, deep), jnp.float32),
            pltpu.VMEM((1, half), jnp.float32),
            pltpu.VMEM((1, half), jnp.float32),
            pltpu.VMEM((1, vsize), jnp.float32),
            pltpu.VMEM((3, channels), jnp.float32),
            pltpu.VMEM((pairs, rows, 2 * w_rows), jnp.float32),
            pltpu.VMEM((n, w_rows, columns), bf16),
            pltpu.VMEM((n * fs * w_rows, columns), bf16),
            pltpu.VMEM((rows, deep), bf16),
            pltpu.VMEM((rows, deep), bf16),
            pltpu.VMEM((tp, total, deep), bf16),
            pltpu.VMEM((w_rows, hidden), bf16),
            pltpu.VMEM((pairs, hidden, 2 * w_rows), bf16),
            pltpu.VMEM((2, total, 2 * half), bf16),
            pltpu.VMEM((total, 2 * half), bf16),
            pltpu.VMEM((total, vsize), bf16),
            pltpu.VMEM((total, channels), bf16),
            pltpu.VMEM((total + 16, channels), jnp.float32),
            pltpu.VMEM((total, channels), bf16),
            pltpu.VMEM((total, vsize), bf16),
            pltpu.VMEM((rows, hidden), bf16),
            pltpu.VMEM((pairs, rows, 2 * w_rows), bf16),
            pltpu.VMEM((2, total, 1), jnp.float32),
            pltpu.VMEM((2, total, 1), jnp.float32),
            pltpu.VMEM((2, total, vsize), jnp.float32),
            dma((n * 6 + 8,)),
            dma((n,)), dma((n,)), dma((2, n)), dma((2, n)), dma((n,)), dma((n,)),
            dma((1,)), dma((1,)), dma((2, n)), dma((n,)), dma((n,)), dma((n,)),
            dma((2, n)), dma((n,)), dma((2, n)), dma((2, n)), dma((2, n)), dma((2, n)),
            dma((n,)), dma((n,)), dma((n,)), dma((n,)), dma((pairs,)), dma((pairs,)), dma((pairs,)),
        ],
        compiler_params=pltpu.CompilerParams(
            collective_id=1, has_side_effects=True, vmem_limit_bytes=60 * 2**20
        ),
    )(
        tokens, query_weight, key_weight, value_weight, post_gate_weight, pre_gate_weight,
        inner_weight, attn_out_weight, conv_out_weight,
        norm_gain.reshape(tp, 1, deep),
        query_gain[None],
        key_gain[None],
        mix_lambda,
        head_gain[None],
        conv_taps,
    )
    return (mine.astype(jnp.float32) + take.astype(jnp.float32)).astype(bf16)[None]


def per_device(
    inputs,
    norm_gain,
    query_weight,
    key_weight,
    value_weight,
    query_gain,
    key_gain,
    mix_lambda,
    head_gain,
    post_gate_weight,
    pre_gate_weight,
    inner_weight,
    conv_taps,
    attn_out_weight,
    conv_out_weight,
):
    tokens = inputs[0]
    whole = lax.all_gather(tokens, "tp", axis=1, tiled=True)
    normed = scale_rows(whole.astype(jnp.float32), norm_gain).astype(jnp.bfloat16)
    heads_dev = value_weight.shape[1] // head_gain.shape[0]
    channels = post_gate_weight.shape[1]
    tp_index = lax.axis_index("tp")
    weight_two = lax.dynamic_slice_in_dim(mix_lambda, tp_index * heads_dev, heads_dev)
    taps = lax.dynamic_slice_in_dim(conv_taps, tp_index * channels, channels, 1)
    every_full = (
        lax.all_gather(query_weight, ("sp", "fs"), axis=0, tiled=True),
        lax.all_gather(key_weight, ("sp", "fs"), axis=0, tiled=True),
        lax.all_gather(value_weight, ("sp", "fs"), axis=0, tiled=True),
        lax.all_gather(post_gate_weight, ("sp", "fs"), axis=0, tiled=True),
        lax.all_gather(pre_gate_weight, ("sp", "fs"), axis=0, tiled=True),
        lax.all_gather(inner_weight, ("sp", "fs"), axis=0, tiled=True),
        lax.all_gather(attn_out_weight, ("sp", "fs"), axis=0, tiled=True),
        lax.all_gather(conv_out_weight, ("sp", "fs"), axis=0, tiled=True),
    )
    query, key, value_proj, post, pre_gate, inner, attn_out_full, conv_out_full = project_all(
        normed, every_full[0:3] + every_full[3:6] + every_full[6:8], 6
    )
    attn_hidden = attention_branch(
        query, key, value_proj.astype(jnp.bfloat16), weight_two, query_gain, key_gain, head_gain
    )
    post_mid = post.astype(jnp.bfloat16)
    post_wide = lax.optimization_barrier(post_mid).astype(jnp.float32)
    signal = (pre_gate * inner).astype(jnp.bfloat16)
    padded = padded_2(signal, (("sp", 0),), 1)
    shifted = lax.optimization_barrier(padded).astype(jnp.float32)
    filtered = taps[0] * shifted[:-2] + taps[1] * shifted[1:-1] + taps[2] * shifted[2:]
    conv_hidden = (post_wide * filtered).astype(jnp.bfloat16)
    contract = (((1,), (1,)), ((), ()))
    summed = lax.psum_scatter(
        (
            lax.dot_general(
                attn_hidden, attn_out_full, contract, preferred_element_type=jnp.float32
            )
            + lax.dot_general(
                conv_hidden, conv_out_full, contract, preferred_element_type=jnp.float32
            )
        ).astype(jnp.bfloat16),
        "tp",
        scatter_dimension=0,
        tiled=True,
    )
    return summed[None]


def solution(mesh):
    placed = (
        P("fs", "sp", "tp"),
        P(),
        P(("sp", "fs"), "tp"),
        P(("sp", "fs"), "tp"),
        P(("sp", "fs"), "tp"),
        P(),
        P(),
        P(),
        P(),
        P(("sp", "fs"), "tp"),
        P(("sp", "fs"), "tp"),
        P(("sp", "fs"), "tp"),
        P(),
        P(("sp", "fs"), "tp"),
        P(("sp", "fs"), "tp"),
    )
    sp, tp = mesh.shape["sp"], mesh.shape["tp"]

    def program(*args):
        heads = args[7].shape[0]
        channels = args[12].shape[1]
        splits = tp == 2 and mesh.shape["fs"] == 4 and sp > 1 and heads == sp * tp
        splits = splits and channels % (sp * tp * 128) == 0
        return shard(split_device if splits else per_device)(*args)

    shard = lambda body: jax.shard_map(
        body,
        mesh=mesh,
        in_specs=placed,
        out_specs=P("fs", ("sp", "tp"), None),
        check_vma=False,
    )

    return program
```

```python
import math

import jax
import jax.numpy as jnp
from jax import lax
from jax.experimental import pallas as pl
from jax.experimental.pallas import tpu as pltpu
from jax.sharding import PartitionSpec as P

epsilon = 1e-06


def padded_2(x, sides, width):
    for axis, dim in sides:
        size, length = (lax.axis_size(axis), x.shape[dim])
        up = [(i, (i + 1) % size) for i in range(size - 1)]
        down = [(j, i) for i, j in up]
        last = lax.slice_in_dim(x, length - width, length, axis=dim)
        initial = lax.slice_in_dim(x, 0, width, axis=dim)
        before = lax.ppermute(last, axis, up)
        after = lax.ppermute(initial, axis, down)
        x = jnp.concatenate([before, x, after], axis=dim)
    return x


def scale_rows(values, gain):
    return values * lax.rsqrt(jnp.mean(values * values, axis=-1, keepdims=True) + epsilon) * gain


def project_all(normed, weights, products):
    result = []
    for member in range(len(weights)):
        if member < products:
            result.append(jnp.dot(normed, weights[member], preferred_element_type=jnp.float32))
        else:
            result.append(weights[member])
    return tuple(result)


def attention_branch(query, key, values, weight_two, query_gain, key_gain, head_gain):
    tok_rows = query.shape[0]
    vsize = head_gain.shape[0]
    half = query_gain.shape[0]
    heads = values.shape[1] // vsize
    query_normed = scale_rows(query.reshape(tok_rows, heads, 2, half), query_gain).astype(
        jnp.bfloat16
    )
    key_normed = scale_rows(key.reshape(tok_rows, heads * 2, half), key_gain).astype(jnp.bfloat16)
    key_normed = key_normed.reshape(tok_rows, heads * 2 * half)
    scale = half ** (-0.5)
    initial = (
        jnp.full((heads, 2, tok_rows), -1e30, jnp.float32),
        jnp.zeros((heads, 2, tok_rows), jnp.float32),
        jnp.zeros((heads, 2, tok_rows, vsize), jnp.float32),
    )
    carry = initial
    key_piece = lax.all_gather(key_normed, "sp", axis=0, tiled=True)
    value_piece = lax.all_gather(values, "sp", axis=0, tiled=True)
    length = key_piece.shape[0]
    block = math.gcd(length, 512)
    key_blocks = key_piece.reshape(length // block, block, heads, 2, half)
    value_blocks = value_piece.reshape(length // block, block, heads, vsize)

    def one_block(state, blocks):
        peak, total, accum = state
        key_block, value_block = blocks
        scores = (
            jnp.einsum(
                "qhjd,khjd->hjqk", query_normed, key_block, preferred_element_type=jnp.float32
            )
            * scale
        )
        new_peak = jnp.maximum(peak, jnp.max(scores, axis=-1))
        factor = jnp.exp(peak - new_peak)
        expo = jnp.exp(scores - new_peak[..., None])
        total = total * factor + jnp.sum(expo, axis=-1)
        accum = accum * factor[..., None] + jnp.einsum(
            "hjqk,khd->hjqd",
            expo.astype(jnp.bfloat16),
            value_block,
            preferred_element_type=jnp.float32,
        )
        return ((new_peak, total, accum), None)

    carry, unused = lax.scan(one_block, carry, (key_blocks, value_blocks))
    peak, total, accum = carry
    mapped = accum / total[..., None]
    head_out = mapped[:, 0] - weight_two[:, None, None] * mapped[:, 1]
    normed_out = scale_rows(head_out, head_gain).astype(jnp.bfloat16)
    return jnp.transpose(normed_out, (1, 0, 2)).reshape(tok_rows, heads * vsize)


def half_scaled(values, gain, half):
    low = lax.broadcasted_iota(jnp.int32, (1, 2 * half), 1) < half
    squares = values * values
    first = jnp.sum(jnp.where(low, squares, 0.0), axis=-1, keepdims=True) / half
    second = jnp.sum(jnp.where(low, 0.0, squares), axis=-1, keepdims=True) / half
    factor = jnp.where(low, lax.rsqrt(first + epsilon), lax.rsqrt(second + epsilon))
    return values * factor * gain


def remote(source, target, send, recv, where):
    return pltpu.make_async_remote_copy(
        src_ref=source,
        dst_ref=target,
        send_sem=send,
        recv_sem=recv,
        device_id=where,
        device_id_type=pl.DeviceIdType.MESH,
    )


def meet(places):
    barrier = pltpu.get_barrier_semaphore()
    for where in places:
        pl.semaphore_signal(
            barrier, inc=1, device_id=where, device_id_type=pl.DeviceIdType.MESH
        )
    pl.semaphore_wait(barrier, len(places))


def load(source, target, sem):
    return pltpu.make_async_copy(source, target, sem)


def choose(table, z):
    value = table[0]
    for at in range(1, len(table)):
        value = jnp.where(z == at, table[at], value)
    return value


def fused_kernel(
    n, half, tok_ref, q_ref, k_ref, v_ref, post_ref, pre_ref, inner_ref, ao_ref, co_ref,
    ng_any, qg_any, kg_any, lam_ref, hg_any, taps_any, mine, take,
    gain_ref, qg_ref, kg_ref, hg_ref, taps_ref, acc, pack, w_all, t_raw, t_twin, t_all, o_raw, wo_all, query, key, val, post, signal, conv_hid,
    attn_hid, hin, both, part_peak, part_total, part_sum,
    l_sem, z_send, z_recv, f_send, f_recv, g_send, g_recv, r_send, r_recv, t_send, t_recv,
    p_send, p_recv, o_send, o_recv, of_send, of_recv, og_send, og_recv, c_send, c_recv,
    a_send, a_recv, e_send, e_recv, s_sem,
):
    z, f, c = lax.axis_index("sp"), lax.axis_index("fs"), lax.axis_index("tp")
    beside, above = f + 1 - 2 * (f % 2), f + 2 - 4 * (f // 2)
    near = sorted(range(1, n), key=lambda d: min(d, n - d))
    fs = 2 * wo_all.shape[0] // n
    rows = tok_ref.shape[0]
    w_rows = q_ref.shape[0]
    total_rows = rows * n
    vsize = v_ref.shape[1] // n
    channels = post_ref.shape[1] // n
    wide = 2 * half
    o_attn = ao_ref.shape[1]
    bf16, f32 = jnp.bfloat16, jnp.float32

    members = ((q_ref, wide), (k_ref, wide), (pre_ref, channels), (inner_ref, channels),
               (post_ref, channels), (v_ref, vsize))
    starts = [0]
    for ref, width in members:
        starts.append(starts[-1] + width)

    def w_place(s, g):
        return w_all.at[pl.ds(pl.multiple_of((s * fs + g) * w_rows, w_rows), w_rows)]

    tok_load = load(tok_ref, t_raw, l_sem.at[n * 6])
    tok_load.start()
    loads = {}
    for d in near + [0]:
        to = (z + d) % n
        target = pack.at[d] if d else w_place(z, f)
        loads[d] = []
        for m, (ref, width) in enumerate(members):
            piece = load(
                ref.at[:, pl.ds(pl.multiple_of(to * width, width), width)],
                target.at[:, pl.ds(starts[m], width)],
                l_sem.at[d * 6 + m],
            )
            piece.start()
            loads[d].append(piece)
    o_loads = [
        load(ao_ref, o_raw.at[:, pl.ds(0, o_attn)], l_sem.at[n * 6 + 1]),
        load(co_ref, o_raw.at[:, pl.ds(o_attn, co_ref.shape[1])], l_sem.at[n * 6 + 2]),
    ]
    place = c * n + z
    small = [
        load(source, target, l_sem.at[n * 6 + 3 + at])
        for at, (source, target) in enumerate((
            (ng_any, gain_ref), (qg_any, qg_ref), (kg_any, kg_ref), (hg_any, hg_ref),
            (taps_any.at[:, pl.ds(pl.multiple_of(place * channels, channels), channels)], taps_ref),
        ))
    ]
    for piece in o_loads + small:
        piece.start()

    meet([{"sp": (z + d) % n} for d in near] + [{"fs": beside}, {"fs": above}, {"tp": 1 - c}])

    flights = []

    def go(copy):
        copy.start()
        flights.append(copy)
        return copy

    tok_load.wait()
    raw = go(remote(t_raw, t_twin, r_send.at[0], r_recv.at[0], {"tp": 1 - c}))
    across = {}
    for d in near:
        for piece in loads[d]:
            piece.wait()
        across[d] = go(
            remote(pack.at[d], w_place(z, f), z_send.at[d], z_recv.at[d], {"sp": (z + d) % n})
        )
    for piece in loads[0]:
        piece.wait()
    side = {}

    def spread(d):
        s = (z + n - d) % n
        for i, to in enumerate((beside, above)):
            side[i, d] = go(
                remote(w_place(s, f), w_place(s, f), f_send.at[i, d], f_recv.at[i, d], {"fs": to})
            )

    further = {}

    def pass_on(d):
        s = (z + n - d) % n
        i = d % 2
        side[i, d].wait_recv()
        held, to = (beside, above) if i == 0 else (above, beside)
        further[d] = go(
            remote(w_place(s, held), w_place(s, held), g_send.at[d], g_recv.at[d], {"fs": to})
        )

    spread(0)

    for piece in small:
        piece.wait()
    raw.wait_recv()
    tile = math.gcd(rows, 64)

    def norm_rows(i, unused):
        at = pl.ds(pl.multiple_of(i * tile, tile), tile)
        to = pl.ds(pl.multiple_of(z * rows + i * tile, tile), tile)
        own, twin = t_raw[at, :].astype(f32), t_twin[at, :].astype(f32)
        square = jnp.sum(own * own, axis=-1, keepdims=True) + jnp.sum(
            twin * twin, axis=-1, keepdims=True
        )
        factor = lax.rsqrt(square / (2 * own.shape[1]) + epsilon)
        t_all[c, to, :] = (own * factor * gain_ref[c]).astype(bf16)
        t_all[1 - c, to, :] = (twin * factor * gain_ref[1 - c]).astype(bf16)
        return unused

    lax.fori_loop(0, rows // tile, norm_rows, 0)

    def t_place(s):
        return t_all.at[c, pl.ds(pl.multiple_of(s * rows, rows), rows)]

    def t_along(s, step):
        return remote(
            t_place(s), t_place(s), t_send.at[(step + 1) // 2, s], t_recv.at[s], {"sp": z + step}
        )

    def t_aside(s):
        return remote(t_place(s), t_place(s), p_send.at[s], p_recv.at[s], {"tp": 1 - c})

    def o_place(s, g):
        at = s * fs + g
        return wo_all.at[at // 2, :, pl.ds(pl.multiple_of(at % 2 * w_rows, w_rows), w_rows)]

    def o_along(s, step):
        return remote(
            o_place(s, f), o_place(s, f), o_send.at[(step + 1) // 2, s], o_recv.at[s],
            {"sp": z + step},
        )

    def o_side(s, i):
        return remote(
            o_place(s, f), o_place(s, f), of_send.at[i, s], of_recv.at[i, s],
            {"fs": (beside, above)[i]},
        )

    def o_further(s, part):
        held, to = (beside, above) if part == 0 else (above, beside)
        at, size = s * fs + held, wo_all.shape[1] // 2
        block = wo_all.at[
            at // 2, pl.ds(part * size, size),
            pl.ds(pl.multiple_of(at % 2 * w_rows, w_rows), w_rows),
        ]
        return remote(block, block, og_send.at[part, s], og_recv.at[part, s], {"fs": to})

    def both_ways(along):
        for step in (1, -1):
            @pl.when(jnp.logical_and(z + step >= 0, z + step < n))
            def _(step=step):
                along(z, step).start()

    both_ways(t_along)

    for piece in o_loads:
        piece.wait()
    square = o_raw.shape[0]
    for i in range(o_raw.shape[1] // square):
        wo_all[
            (z * fs + f) // 2, i * square:(i + 1) * square,
            pl.ds(pl.multiple_of(f % 2 * w_rows, w_rows), w_rows),
        ] = o_raw[:, i * square:(i + 1) * square].T
    both_ways(o_along)

    last = 0
    for d in near:
        across[d].wait_recv()
        spread(d)
        pass_on(last)
        last = d
    pass_on(last)
    for i in range(2):
        o_side(z, i).start()
    for d in range(n):
        side[1 - d % 2, d].wait_recv()
        further[d].wait_recv()

    order = [sorted(range(n), key=lambda s: (abs(s - at), s > at if 2 * at < n else s < at))
             for at in range(n)]

    def t_event(at, s):
        t_along(s, 1).wait_recv()
        step = 1 if s < at else -1
        if 0 <= at + step < n:
            t_along(s, step).start()
        t_aside(s).start()

    def o_event(at, s):
        o_along(s, 1).wait_recv()
        step = 1 if s < at else -1
        if 0 <= at + step < n:
            o_along(s, step).start()
        for i in range(2):
            o_side(s, i).start()

    def o_pass(at, s):
        for part in range(2):
            o_side(s, part).wait_recv()
            o_further(s, part).start()

    plans = []
    for at in range(n):
        plan, t_done, o_done, passed = [], {at}, [at], []
        for visit in range(1, n):
            events, held = [], [r for r in o_done if r not in passed]
            s = order[at][visit]
            if s not in t_done:
                ring = [r for r in order[at] if abs(r - at) == abs(s - at)]
                events += [(t_event, r) for r in ring]
                t_done |= set(ring)
                if visit + len(ring) < n:
                    events += [(o_event, r) for r in ring]
                    o_done += ring
            passes = [(o_pass, r) for r in held]
            plan.append(passes + events if visit == n - 1 else events + passes)
            passed += held
        plan.append([(o_event, r) for r in order[at] if r not in o_done])
        plan.append([(o_pass, r) for r in order[at] if r not in passed])
        plans.append(plan)

    def follow(events):
        for at in range(n):
            if events(at):
                @pl.when(z == at)
                def _(at=at):
                    for event, s in events(at):
                        event(at, s)

    deep = t_all.shape[2]
    m_rows = math.gcd(rows, 256)

    q_gain = jnp.concatenate([qg_ref[...], qg_ref[...]], axis=1)
    k_gain = jnp.concatenate([kg_ref[...], kg_ref[...]], axis=1)

    def project(s):
        def some(i, unused):
            base = pl.multiple_of(s * rows + i * m_rows, m_rows)
            at = pl.ds(base, m_rows)

            def product(first, final):
                lo, hi = starts[first], starts[final]
                return jnp.dot(
                    t_all[0, at, :], w_all[0:deep, lo:hi], preferred_element_type=f32
                ) + jnp.dot(
                    t_all[1, at, :], w_all[deep:2 * deep, lo:hi], preferred_element_type=f32
                )

            pair = product(0, 2)
            low = lax.broadcasted_iota(jnp.int32, (1, wide), 1) < half
            q = half_scaled(pair[:, :wide], q_gain, half).astype(bf16).astype(f32)
            query[0, at, :] = jnp.where(low, q, 0.0).astype(bf16)
            query[1, at, :] = jnp.where(low, 0.0, q).astype(bf16)
            key[at, :] = half_scaled(pair[:, wide:], k_gain, half).astype(bf16)
            mixed = product(2, 3) * product(3, 4)
            signal[pl.ds(base + 8, m_rows), :] = mixed.astype(bf16).astype(f32)
            post[at, :] = product(4, 5).astype(bf16)
            val[at, :] = product(5, 6).astype(bf16)
            return unused

        lax.fori_loop(0, rows // m_rows, some, 0)

    signal[0:8, :] = jnp.zeros((8, channels), f32)
    signal[total_rows + 8:total_rows + 16, :] = jnp.zeros((8, channels), f32)
    h_rows = math.gcd(rows, 64)
    conv_at = pl.ds(pl.multiple_of(o_attn + z * channels, channels), channels)
    attn_at = pl.ds(pl.multiple_of(z * vsize, vsize), vsize)
    own = pl.ds(pl.multiple_of(z * rows, rows), rows)

    def convolve(s):
        def some(i, unused):
            base = pl.multiple_of(s * rows + i * h_rows, h_rows)
            around = signal[pl.ds(base, h_rows + 16), :]
            filtered = (
                taps_ref[0:1] * around[7:7 + h_rows]
                + taps_ref[1:2] * around[8:8 + h_rows]
                + taps_ref[2:3] * around[9:9 + h_rows]
            )
            at = pl.ds(base, h_rows)
            conv_hid[at, :] = (post[at, :].astype(f32) * filtered).astype(bf16)
            return unused

        lax.fori_loop(0, rows // h_rows, some, 0)

    def sent_to(source, columns, to, send, recv):
        return remote(
            source.at[pl.ds(pl.multiple_of(to * rows, rows), rows)], hin.at[:, columns],
            send.at[to], recv.at[z], {"sp": to},
        )

    def c_copy(to):
        return sent_to(conv_hid, conv_at, to, c_send, c_recv)

    def a_copy(to):
        return sent_to(attn_hid, attn_at, to, a_send, a_recv)

    def convolve_send(s):
        @pl.when(s != z)
        def _():
            c_copy(s).start()

    whole = []
    for at in range(n):
        seen, out, stages = {at}, set(), []
        for visit in range(1, n):
            seen.add(order[at][visit])
            fresh = [r for r in order[at] if r not in out
                     and all(q in seen for q in (r - 1, r, r + 1) if 0 <= q < n)]
            out |= set(fresh)
            stages.append(fresh)
        whole.append(stages)
    counts = [max(len(whole[at][v]) for at in range(n)) for v in range(n - 1)]

    def each_whole(visit, act):
        for k in range(counts[visit - 1]):
            held = [whole[at][visit - 1] for at in range(n)]
            s = choose([p[k] if k < len(p) else -1 for p in held], z)
            if all(k < len(p) for p in held):
                act(s)
            else:
                @pl.when(s >= 0)
                def _(s=s):
                    act(s)

    a_rows = math.gcd(rows, 256)
    each = rows // a_rows
    scale = half ** (-0.5) * math.log2(math.e)
    lam = lam_ref[place]
    is_end = jnp.logical_or(z == 0, z == n - 1)
    final = choose([order[at][n - 1] for at in range(n)], z)

    def compare(which, at, keys):
        return lax.dot_general(
            query[which, at, :], key[keys, :], (((1,), (1,)), ((), ())),
            preferred_element_type=f32,
        ) * scale

    def soft(which, at, keys):
        scores = compare(which, at, keys)
        peak = jnp.max(scores, axis=-1, keepdims=True)
        expo = jnp.exp2(scores - peak)
        total = jnp.sum(expo, axis=-1, keepdims=True)
        return peak, total, jnp.dot(
            expo.astype(bf16), val[keys, :], preferred_element_type=f32
        )

    def attend_first():
        start = jnp.where(final == 0, rows, 0)
        keys = pl.ds(pl.multiple_of(start, rows), total_rows - rows)

        def some(i, unused):
            at = pl.ds(pl.multiple_of(start + i * a_rows, a_rows), a_rows)
            for which in range(2):
                peak, total, accum = soft(which, at, keys)
                part_peak[which, at, :] = peak
                part_total[which, at, :] = total
                part_sum[which, at, :] = accum
            return unused

        lax.fori_loop(0, (n - 1) * each, some, 0)

    project(z)
    for visit in range(1, n):
        if visit == n - 1:
            pl.when(is_end)(attend_first)
        follow(lambda at: plans[at][visit - 1])
        s = choose([order[at][visit] for at in range(n)], z)
        t_aside(s).wait_recv()
        project(s)
        each_whole(visit, convolve)

        @pl.when(is_end)
        def _(visit=visit):
            each_whole(visit, convolve_send)
    hin[:, conv_at] = conv_hid[own, :]
    pl.when(jnp.logical_not(is_end))(attend_first)
    far = near[::-1]

    follow_rest = [lambda at, k=k: plans[at][n - 1 + k] for k in range(2)]

    def attend(i, unused):
        @pl.when(i == jnp.where(is_end, (n * each) // 2, 0))
        def _():
            follow(follow_rest[0])


        @pl.when(jnp.logical_and(i == each, jnp.logical_not(is_end)))
        def _():
            for visit in range(1, n):
                each_whole(visit, convolve_send)

        @pl.when(jnp.logical_and(i == n * each - 2, jnp.logical_not(is_end)))
        def _():
            follow(follow_rest[1])

        block = (z + choose(far + [0], i // each)) % n
        at = pl.ds(pl.multiple_of(block * rows + (i % each) * a_rows, a_rows), a_rows)

        def finish(maps):
            head_out = maps[0] - lam * maps[1]
            attn_hid[at, :] = scale_rows(head_out, hg_ref[...]).astype(bf16)

        @pl.when(block != final)
        def _():
            maps = []
            late = pl.ds(pl.multiple_of(final * rows, rows), rows)
            for which in range(2):
                scores = compare(which, at, late)
                before = part_peak[which, at, :]
                peak = jnp.maximum(before, jnp.max(scores, axis=-1, keepdims=True))
                factor, expo = jnp.exp2(before - peak), jnp.exp2(scores - peak)
                total = part_total[which, at, :] * factor + jnp.sum(expo, axis=-1, keepdims=True)
                accum = part_sum[which, at, :] * factor + jnp.dot(
                    expo.astype(bf16), val[late, :], preferred_element_type=f32
                )
                maps.append(accum / total)
            finish(maps)

        @pl.when(block == final)
        def _():
            maps = []
            for which in range(2):
                unused_peak, total, accum = soft(which, at, pl.ds(0, total_rows))
                maps.append(accum / total)
            finish(maps)

        for j, d in enumerate(far):
            @pl.when(i == (j + 1) * each - 1)
            def _(d=d):
                a_copy((z + d) % n).start()
        return unused

    lax.fori_loop(0, n * each, attend, 0)

    @pl.when(is_end)
    def _():
        follow(follow_rest[1])

    hin[:, attn_at] = attn_hid[own, :]

    def arrived(source, columns, d, send, recv):
        s = (z + d) % n
        remote(
            source.at[pl.ds(0, rows)], hin.at[:, columns], send.at[s], recv.at[s], {"sp": s}
        ).wait_recv()

    for d in near:
        arrived(conv_hid, conv_at, d, c_send, c_recv)

    pairs = wo_all.shape[0]
    half_rows = rows // 2
    width = 2 * w_rows

    theirs = pl.ds(pl.multiple_of((1 - c) * half_rows, half_rows), half_rows)
    ours = pl.ds(pl.multiple_of(c * half_rows, half_rows), half_rows)

    def swap(j):
        at = pl.ds(pl.multiple_of(j * width, width), width)
        return remote(
            both.at[j, theirs], take.at[:, at], e_send.at[j], e_recv.at[j], {"tp": 1 - c}
        )

    def store(j):
        at = pl.ds(pl.multiple_of(j * width, width), width)
        return load(both.at[j, ours], mine.at[:, at], s_sem.at[j])

    def channel_part(j, unused):
        acc[j] = jnp.dot(hin[:, o_attn:], wo_all[j, o_attn:, :], preferred_element_type=f32)
        return unused

    for visit in range(n):
        s = choose([order[at][visit] for at in range(n)], z)
        for part in range(2):
            o_further(s, part).wait_recv()
        lax.fori_loop(s * (fs // 2), (s + 1) * (fs // 2), channel_part, 0)
    for d in near:
        arrived(attn_hid, attn_at, d, a_send, a_recv)

    def head_part(j, unused):
        both[j] = (
            acc[j]
            + jnp.dot(hin[:, :o_attn], wo_all[j, :o_attn, :], preferred_element_type=f32)
        ).astype(bf16)
        swap(j).start()
        store(j).start()
        return unused

    lax.fori_loop(0, pairs, head_part, 0)
    for j in range(pairs):
        swap(j).wait_recv()
        store(j).wait()

    for copy in flights:
        copy.wait_send()
    for d in far:
        c_copy((z + d) % n).wait_send()
        a_copy((z + d) % n).wait_send()
    for j in range(pairs):
        swap(j).wait_send()
    for s in range(n):
        for i in range(2):
            o_side(s, i).wait_send()
            o_further(s, i).wait_send()
        for step in (1, -1):
            arrives = s <= z if step == 1 else s >= z
            @pl.when(jnp.logical_and(arrives, jnp.logical_and(z + step >= 0, z + step < n)))
            def _(s=s, step=step):
                t_along(s, step).wait_send()
                o_along(s, step).wait_send()

        @pl.when(z != s)
        def _(s=s):
            t_aside(s).wait_send()


def split_device(
    inputs,
    norm_gain,
    query_weight,
    key_weight,
    value_weight,
    query_gain,
    key_gain,
    mix_lambda,
    head_gain,
    post_gate_weight,
    pre_gate_weight,
    inner_weight,
    conv_taps,
    attn_out_weight,
    conv_out_weight,
):
    n, fs, tp = lax.axis_size("sp"), lax.axis_size("fs"), lax.axis_size("tp")
    tokens = inputs[0]
    rows, deep = tokens.shape
    half, vsize = query_gain.shape[0], head_gain.shape[0]
    channels = post_gate_weight.shape[1] // n
    w_rows = query_weight.shape[0]
    columns = 4 * half + vsize + 3 * channels
    hidden = n * (vsize + channels)
    total = n * rows
    out_width = w_rows * n * fs
    pairs = n * fs // 2
    bf16, dma = jnp.bfloat16, pltpu.SemaphoreType.DMA
    far = pl.BlockSpec(memory_space=pl.ANY)
    mine, take = pl.pallas_call(
        lambda *refs: fused_kernel(n, half, *refs),
        out_shape=(jax.ShapeDtypeStruct((rows // tp, out_width), bf16),) * 2,
        in_specs=[far] * 12 + [pl.BlockSpec(memory_space=pltpu.SMEM)] + [far] * 2,
        out_specs=(far, far),
        scratch_shapes=[
            pltpu.VMEM((tp, 1, deep), jnp.float32),
            pltpu.VMEM((1, half), jnp.float32),
            pltpu.VMEM((1, half), jnp.float32),
            pltpu.VMEM((1, vsize), jnp.float32),
            pltpu.VMEM((3, channels), jnp.float32),
            pltpu.VMEM((pairs, rows, 2 * w_rows), jnp.float32),
            pltpu.VMEM((n, w_rows, columns), bf16),
            pltpu.VMEM((n * fs * w_rows, columns), bf16),
            pltpu.VMEM((rows, deep), bf16),
            pltpu.VMEM((rows, deep), bf16),
            pltpu.VMEM((tp, total, deep), bf16),
            pltpu.VMEM((w_rows, hidden), bf16),
            pltpu.VMEM((pairs, hidden, 2 * w_rows), bf16),
            pltpu.VMEM((2, total, 2 * half), bf16),
            pltpu.VMEM((total, 2 * half), bf16),
            pltpu.VMEM((total, vsize), bf16),
            pltpu.VMEM((total, channels), bf16),
            pltpu.VMEM((total + 16, channels), jnp.float32),
            pltpu.VMEM((total, channels), bf16),
            pltpu.VMEM((total, vsize), bf16),
            pltpu.VMEM((rows, hidden), bf16),
            pltpu.VMEM((pairs, rows, 2 * w_rows), bf16),
            pltpu.VMEM((2, total, 1), jnp.float32),
            pltpu.VMEM((2, total, 1), jnp.float32),
            pltpu.VMEM((2, total, vsize), jnp.float32),
            dma((n * 6 + 8,)),
            dma((n,)), dma((n,)), dma((2, n)), dma((2, n)), dma((n,)), dma((n,)),
            dma((1,)), dma((1,)), dma((2, n)), dma((n,)), dma((n,)), dma((n,)),
            dma((2, n)), dma((n,)), dma((2, n)), dma((2, n)), dma((2, n)), dma((2, n)),
            dma((n,)), dma((n,)), dma((n,)), dma((n,)), dma((pairs,)), dma((pairs,)), dma((pairs,)),
        ],
        compiler_params=pltpu.CompilerParams(
            collective_id=1, has_side_effects=True, vmem_limit_bytes=60 * 2**20
        ),
    )(
        tokens, query_weight, key_weight, value_weight, post_gate_weight, pre_gate_weight,
        inner_weight, attn_out_weight, conv_out_weight,
        norm_gain.reshape(tp, 1, deep),
        query_gain[None],
        key_gain[None],
        mix_lambda,
        head_gain[None],
        conv_taps,
    )
    return (mine.astype(jnp.float32) + take.astype(jnp.float32)).astype(bf16)[None]


def per_device(
    inputs,
    norm_gain,
    query_weight,
    key_weight,
    value_weight,
    query_gain,
    key_gain,
    mix_lambda,
    head_gain,
    post_gate_weight,
    pre_gate_weight,
    inner_weight,
    conv_taps,
    attn_out_weight,
    conv_out_weight,
):
    tokens = inputs[0]
    whole = lax.all_gather(tokens, "tp", axis=1, tiled=True)
    normed = scale_rows(whole.astype(jnp.float32), norm_gain).astype(jnp.bfloat16)
    heads_dev = value_weight.shape[1] // head_gain.shape[0]
    channels = post_gate_weight.shape[1]
    tp_index = lax.axis_index("tp")
    weight_two = lax.dynamic_slice_in_dim(mix_lambda, tp_index * heads_dev, heads_dev)
    taps = lax.dynamic_slice_in_dim(conv_taps, tp_index * channels, channels, 1)
    every_full = (
        lax.all_gather(query_weight, ("sp", "fs"), axis=0, tiled=True),
        lax.all_gather(key_weight, ("sp", "fs"), axis=0, tiled=True),
        lax.all_gather(value_weight, ("sp", "fs"), axis=0, tiled=True),
        lax.all_gather(post_gate_weight, ("sp", "fs"), axis=0, tiled=True),
        lax.all_gather(pre_gate_weight, ("sp", "fs"), axis=0, tiled=True),
        lax.all_gather(inner_weight, ("sp", "fs"), axis=0, tiled=True),
        lax.all_gather(attn_out_weight, ("sp", "fs"), axis=0, tiled=True),
        lax.all_gather(conv_out_weight, ("sp", "fs"), axis=0, tiled=True),
    )
    query, key, value_proj, post, pre_gate, inner, attn_out_full, conv_out_full = project_all(
        normed, every_full[0:3] + every_full[3:6] + every_full[6:8], 6
    )
    attn_hidden = attention_branch(
        query, key, value_proj.astype(jnp.bfloat16), weight_two, query_gain, key_gain, head_gain
    )
    post_mid = post.astype(jnp.bfloat16)
    post_wide = lax.optimization_barrier(post_mid).astype(jnp.float32)
    signal = (pre_gate * inner).astype(jnp.bfloat16)
    padded = padded_2(signal, (("sp", 0),), 1)
    shifted = lax.optimization_barrier(padded).astype(jnp.float32)
    filtered = taps[0] * shifted[:-2] + taps[1] * shifted[1:-1] + taps[2] * shifted[2:]
    conv_hidden = (post_wide * filtered).astype(jnp.bfloat16)
    contract = (((1,), (1,)), ((), ()))
    summed = lax.psum_scatter(
        (
            lax.dot_general(
                attn_hidden, attn_out_full, contract, preferred_element_type=jnp.float32
            )
            + lax.dot_general(
                conv_hidden, conv_out_full, contract, preferred_element_type=jnp.float32
            )
        ).astype(jnp.bfloat16),
        "tp",
        scatter_dimension=0,
        tiled=True,
    )
    return summed[None]


def solution(mesh):
    placed = (
        P("fs", "sp", "tp"),
        P(),
        P(("sp", "fs"), "tp"),
        P(("sp", "fs"), "tp"),
        P(("sp", "fs"), "tp"),
        P(),
        P(),
        P(),
        P(),
        P(("sp", "fs"), "tp"),
        P(("sp", "fs"), "tp"),
        P(("sp", "fs"), "tp"),
        P(),
        P(("sp", "fs"), "tp"),
        P(("sp", "fs"), "tp"),
    )
    sp, tp = mesh.shape["sp"], mesh.shape["tp"]

    def program(*args):
        heads = args[7].shape[0]
        channels = args[12].shape[1]
        splits = tp == 2 and mesh.shape["fs"] == 4 and sp > 1 and heads == sp * tp
        splits = splits and channels % (sp * tp * 128) == 0
        return shard(split_device if splits else per_device)(*args)

    shard = lambda body: jax.shard_map(
        body,
        mesh=mesh,
        in_specs=placed,
        out_specs=P("fs", ("sp", "tp"), None),
        check_vma=False,
    )

    return program
```
